128 devices in a mesh: grp: 4 (over y, x), ep: 32 (over z, core).
Axes of the slice: x: 2, y: 2, z: 16, core: 2. Of those that a mesh axis runs over, the one named last changes fastest.
The devices are a block of a 8x8x16 slice.
Arguments:
- tokens: bfloat16 [256, 2048], P('grp', 'ep'), parts along dimension 0, may hold values from -6 to 6
- w_query: bfloat16 [2048, 1024], P('ep'), may hold values from -0.125 to 0.125
- w_key: bfloat16 [2048, 1024], P('ep'), may hold values from -0.125 to 0.125
- w_value: bfloat16 [2048, 1024], P('ep'), may hold values from -0.125 to 0.125
- w_forget: bfloat16 [2048, 16], P('ep'), may hold values from -0.125 to 0.125
- forget_bias: float32 [16], replicated, may hold values from -1 to 2
- cache_keys: bfloat16 [256, 1024, 1024], P(('grp', 'ep')), parts along dimension 0
- cache_values: bfloat16 [256, 1024, 1024], P(('grp', 'ep')), parts along dimension 0, may hold values from -6 to 6
- cache_gates: float32 [256, 1024, 16], P(('grp', 'ep')), parts along dimension 0, as said below
- lengths: int32 [256], P(('grp', 'ep')), parts along dimension 0, may hold values from 128 to 1024, as said below
- w_out: bfloat16 [1024, 2048], P('ep'), may hold values from -0.1875 to 0.1875
- norm_gain: bfloat16 [2048], replicated, may hold values from 0.099609375 to 1.8984375
- w_router: bfloat16 [2048, 4], replicated, may hold values from -0.125 to 0.125
- routes: int32 [256, 2], P('grp'), parts along dimension 0, may hold values from 0 to 3, all different within a row
- dense_gate: bfloat16 [2048], replicated, may hold values from -0.25 to 0.25
- dense_w_gate: bfloat16 [2048, 8192], P(None, 'ep'), may hold values from -0.125 to 0.125
- dense_w_up: bfloat16 [2048, 8192], P(None, 'ep'), may hold values from -0.125 to 0.125
- dense_w_down: bfloat16 [8192, 2048], P('ep'), may hold values from -0.125 to 0.125
- expert_w_gate: bfloat16 [2048, 16384], P(None, 'ep'), may hold values from -0.125 to 0.125
- expert_w_up: bfloat16 [2048, 16384], P(None, 'ep'), may hold values from -0.125 to 0.125
- expert_w_down: bfloat16 [16384, 2048], P('ep'), may hold values from -0.1875 to 0.1875
- final_gain: bfloat16 [2048], P('ep'), may hold values from 0.099609375 to 1.8984375
Outputs:
- result: bfloat16 [256, 2048], P('grp', 'ep'), parts along dimension 0
The draws below stay inside these ranges and needn't reach their ends.
There are 4 independent parts, one for each index of `grp`. The reference program is written for one: setup_inputs(seed, part) draws one part's arguments, and reference() takes and returns one part's arrays. A program takes and returns all parts, laid end to end along the dimension named above; an argument that names none is the same for every part. Nothing has to cross between parts.
Inputs may be any that keep to these rules, and one draw needn't show every extreme that they name: `routes`: each row names 2 different experts; every expert is named by some row. `lengths`: the first sequence of each part holds 1024 positions. `cache_gates`: never rising along positions.
All inputs are finite; a program needn't handle non-finite values.
Results may differ from the reference program's by a relative error of at most 0.0085.
Values may be sent and summed in bfloat16 or wider, within the bound.
No kernel may reach another device: no remote copies, remote signals or barrier semaphores. Data moves between devices by JAX's collectives and lax.ppermute only.
A program may use at most 128 MiB of HBM per device.

```python
import jax
import jax.numpy as jnp
from jax import lax

D = 2048
QUERY_GROUPS = 16
ATT = 1024
BATCH_LENGTH = 64
STORED_PLACES = 1024
EXPERT_FF = 4096
EXPERTS = 4
TOPK = 2
DENSE_FF = 8192


def draw_lengths(key, part):
    picked = jax.random.randint(jax.random.fold_in(key, 11), (BATCH_LENGTH,), STORED_PLACES // 8, STORED_PLACES + 1)
    return picked.at[0].set(STORED_PLACES).astype(jnp.int32)


def draw_cache_keys(key, part):
    base = jax.random.normal(jax.random.fold_in(key, 21), (BATCH_LENGTH, STORED_PLACES, ATT), jnp.float32)
    return base.astype(jnp.bfloat16)


def draw_cache_gates(key, part):
    lookup_matrix = jax.random.split(jax.random.fold_in(key, 31), 7)
    slow_share = 0.5
    lagging_portion = jax.random.uniform(lookup_matrix[0], (QUERY_GROUPS,), jnp.float32) < slow_share
    seq_factor = jnp.exp(jax.random.uniform(lookup_matrix[1], (BATCH_LENGTH, 1, 1), jnp.float32, -0.7, 0.7))
    pos_factor = jax.random.uniform(lookup_matrix[2], (BATCH_LENGTH, STORED_PLACES, 1), jnp.float32, 0.5, 1.5)
    slow_rate = jax.random.uniform(lookup_matrix[3], (BATCH_LENGTH, 1, QUERY_GROUPS), jnp.float32, 0.5, 2.0) / STORED_PLACES
    fast_rate = jax.random.uniform(lookup_matrix[4], (BATCH_LENGTH, 1, QUERY_GROUPS), jnp.float32, 1.0 / 100.0, 1.0 / 30.0)
    fading_speed = jnp.where(lagging_portion[None, None, :], slow_rate, fast_rate) * seq_factor * pos_factor
    spike_quantity = jax.random.uniform(lookup_matrix[5], (BATCH_LENGTH, STORED_PLACES, QUERY_GROUPS), jnp.float32) < 3.0 / STORED_PLACES
    shrink_multiplier = jnp.log(jax.random.uniform(lookup_matrix[6], (BATCH_LENGTH, STORED_PLACES, QUERY_GROUPS), jnp.float32, 0.5, 0.8))
    forget_each_token = -fading_speed + jnp.where(jnp.logical_and(spike_quantity, lagging_portion[None, None, :]), shrink_multiplier, 0.0)
    return jnp.cumsum(forget_each_token, axis=1).astype(jnp.float32)


def spiked(result, key, source, target, blocks, factor):
    def block_of(axis_at):
        return (jnp.arange(result.shape[axis_at]) // (result.shape[axis_at] // blocks)).reshape((-1,) + (1,) * (result.ndim - 1 - axis_at))

    one_side = jax.random.permutation(key, blocks)[block_of(target)]
    second = (block_of(target) + blocks // 2) % blocks
    return jnp.where((block_of(source) == one_side) | (block_of(source) == second), factor * result, result)


def levels(key, shape, cuts, smallest, high):
    def one(dim, blocks):
        draws = jax.random.uniform(jax.random.fold_in(jax.random.fold_in(key, 6), dim), (blocks,), jnp.float32, smallest / len(cuts), high / len(cuts))
        return jnp.repeat(jnp.exp(draws), shape[dim] // blocks).reshape((-1,) + (1,) * (len(shape) - dim - 1))

    level = one(*cuts[0])
    for cut in cuts[1:]:
        level = level * one(*cut)
    return level


def distinct(rng, rows, count, top, lift):
    ranking = jax.random.permutation(jax.random.fold_in(rng, 1), count)
    favour = ranking
    for power in range(3):
        favour = favour * favour // count
    favour = favour * lift // count
    chance = jax.random.randint(jax.random.fold_in(rng, 2), (rows, count), 0, 4096) + favour
    holders = jax.random.permutation(jax.random.fold_in(rng, 3), rows)[jnp.arange(count) % rows]
    chance = jnp.where(jnp.arange(rows)[:, None] == holders[None, :], 1 << 14, chance)
    merit = chance * count + jnp.arange(count)
    return lax.top_k(merit.astype(jnp.int32), top)[1].astype(jnp.int32)


def scatter_about(key, extent, spread, most, shards=(), kind=jnp.bfloat16):
    entries = jax.random.normal(key, extent, jnp.float32) * spread
    if len(shards) > 0:
        entries = levels(key, extent, shards, -0.22, 0.18) * entries
    return jnp.clip(entries, min=-most, max=most).astype(kind)


def noise_with(rng, shape, scale, limit, pieces, heavy, held_as=jnp.bfloat16):
    entries = scale * jax.random.normal(rng, shape, jnp.float32)
    if pieces:
        entries = entries * levels(rng, shape, pieces, -0.22, 0.18)
    return jnp.clip(spiked(entries, jax.random.fold_in(rng, 3), *heavy), -limit, limit).astype(held_as)


def setup_inputs(seed: int = 0, part: int = 0) -> dict:
    keys = jax.random.split(jax.random.key(seed), 23)
    part_keys = jax.random.split(jax.random.fold_in(keys[22], part), 23)
    tokens = noise_with(part_keys[0], (BATCH_LENGTH, D), 1.0, 6.0, ((1, 32),), (1, 0, 32, 2.75))
    w_query = scatter_about(keys[1], (D, ATT), D ** -0.5, 0.125, ((0, 32),))
    w_key = scatter_about(keys[2], (D, ATT), D ** -0.5, 0.125, ((0, 32),))
    w_value = scatter_about(keys[3], (D, ATT), D ** -0.5, 0.125, ((0, 32),))
    w_forget = scatter_about(keys[4], (D, QUERY_GROUPS), D ** -0.5, 0.125, ((0, 32),))
    forget_bias = jnp.clip(jax.random.uniform(keys[5], (QUERY_GROUPS,), jnp.float32, -1.0, 2.0), -1.0, 2.0)
    cache_keys = draw_cache_keys(jax.random.fold_in(jax.random.fold_in(keys[22], part), 71), part)
    cache_values = scatter_about(part_keys[7], (BATCH_LENGTH, STORED_PLACES, ATT), 1.0, 6.0, ((0, 32),))
    cache_gates = draw_cache_gates(jax.random.fold_in(jax.random.fold_in(keys[22], part), 71), part)
    lengths = draw_lengths(jax.random.fold_in(jax.random.fold_in(keys[22], part), 71), part)
    w_out = scatter_about(keys[10], (ATT, D), ATT ** -0.5, 0.1875, ((0, 32),))
    norm_gain = jnp.clip(1.0 + 0.18 * jax.random.normal(keys[11], (D,), jnp.float32), 0.099609375, 1.8984375).astype(jnp.bfloat16)
    w_router = scatter_about(keys[12], (D, EXPERTS), D ** -0.5, 0.125)
    routes = distinct(part_keys[13], BATCH_LENGTH, EXPERTS, TOPK, 4096)
    dense_gate = scatter_about(keys[14], (D,), (D // 4) ** -0.5, 0.25)
    dense_w_gate = scatter_about(keys[15], (D, DENSE_FF), D ** -0.5, 0.125, ((1, 32),))
    dense_w_up = scatter_about(keys[16], (D, DENSE_FF), D ** -0.5, 0.125, ((1, 32),))
    dense_w_down = noise_with(keys[17], (DENSE_FF, D), DENSE_FF ** -0.5, 0.125, ((0, 32),), (0, 1, 32, 2.75))
    expert_w_gate = scatter_about(keys[18], (D, EXPERTS * EXPERT_FF), D ** -0.5, 0.125, ((1, 32),))
    expert_w_up = scatter_about(keys[19], (D, EXPERTS * EXPERT_FF), D ** -0.5, 0.125, ((1, 32),))
    expert_w_down = noise_with(keys[20], (EXPERTS * EXPERT_FF, D), EXPERT_FF ** -0.5, 0.1875, ((0, 32),), (0, 1, 32, 2.75))
    final_gain = jnp.clip(1.0 + 0.18 * jax.random.normal(keys[21], (D,), jnp.float32), 0.099609375, 1.8984375).astype(jnp.bfloat16)
    return dict(tokens=tokens, w_query=w_query, w_key=w_key, w_value=w_value, w_forget=w_forget, forget_bias=forget_bias, cache_keys=cache_keys, cache_values=cache_values, cache_gates=cache_gates, lengths=lengths, w_out=w_out, norm_gain=norm_gain, w_router=w_router, routes=routes, dense_gate=dense_gate, dense_w_gate=dense_w_gate, dense_w_up=dense_w_up, dense_w_down=dense_w_down, expert_w_gate=expert_w_gate, expert_w_up=expert_w_up, expert_w_down=expert_w_down, final_gain=final_gain)


norm_eps = 1e-05
residual_scale = 8.0 ** 0.25

def norm_rows(values, weights):
    center = lax.optimization_barrier(jnp.mean(values, axis=-1, keepdims=True))
    second = lax.optimization_barrier(jnp.mean(values * values, axis=-1, keepdims=True))
    return (values - center) * lax.rsqrt(second - center * center + norm_eps) * weights.astype(jnp.float32)

def attend(query, new_key, new_value, forget_pre, forget_bias, cache_keys, cache_values, cache_gates, lengths):
    seqs_here, width = query.shape
    heads = cache_gates.shape[2]
    head_size = width // heads
    cache_len = cache_keys.shape[1]
    query = query.reshape(seqs_here, heads, head_size).astype(jnp.float32)
    new_key = new_key.reshape(seqs_here, heads, head_size).astype(jnp.float32)
    new_value = new_value.reshape(seqs_here, heads, head_size).astype(jnp.float32)
    keys_all = cache_keys.reshape(seqs_here, cache_len, heads, head_size).astype(jnp.float32)
    values_all = cache_values.reshape(seqs_here, cache_len, heads, head_size).astype(jnp.float32)
    log_gate = jax.nn.log_sigmoid(forget_pre + forget_bias[None, :])
    position = jnp.arange(cache_len, dtype=jnp.int32)
    is_last = (position[None, :] == (lengths - 1)[:, None]).astype(jnp.float32)
    last_gate = lax.optimization_barrier(jnp.sum(cache_gates * is_last[:, :, None], axis=1))
    bias = (last_gate + log_gate)[:, :, None] - jnp.transpose(cache_gates, (0, 2, 1))
    scale = head_size ** (-0.5)
    scores = jnp.einsum('shd,slhd->shl', query, keys_all) * scale + bias
    valid = (position[None, :] < lengths[:, None])[:, None, :]
    scores = jnp.where(valid, scores, -jnp.inf)
    own_score = lax.optimization_barrier(jnp.sum(query * new_key, axis=-1)) * scale
    top = jnp.maximum(lax.optimization_barrier(jnp.max(scores, axis=-1)), own_score)
    weights_cache = jnp.exp(scores - top[:, :, None])
    weight_own = jnp.exp(own_score - top)
    total = lax.optimization_barrier(jnp.sum(weights_cache, axis=-1)) + weight_own
    probs = (weights_cache / total[:, :, None]).astype(jnp.bfloat16)
    prob_own = (weight_own / total).astype(jnp.bfloat16)
    mixed = jnp.einsum('shl,slhd->shd', probs.astype(jnp.float32), values_all)
    mixed = mixed + prob_own.astype(jnp.float32)[:, :, None] * new_value
    return mixed.astype(jnp.bfloat16).reshape(seqs_here, width)

def reference(tokens, w_query, w_key, w_value, w_forget, forget_bias, cache_keys, cache_values, cache_gates, lengths, w_out, norm_gain, w_router, routes, dense_gate, dense_w_gate, dense_w_up, dense_w_down, expert_w_gate, expert_w_up, expert_w_down, final_gain):
    query = jnp.dot(tokens, w_query, preferred_element_type=jnp.float32).astype(jnp.bfloat16)
    new_key = jnp.dot(tokens, w_key, preferred_element_type=jnp.float32).astype(jnp.bfloat16)
    new_value = jnp.dot(tokens, w_value, preferred_element_type=jnp.float32).astype(jnp.bfloat16)
    forget_pre = jnp.dot(tokens, w_forget, preferred_element_type=jnp.float32)
    attn = attend(query, new_key, new_value, forget_pre, forget_bias, cache_keys, cache_values, cache_gates, lengths)
    mixed = residual_scale * tokens.astype(jnp.float32) + jnp.dot(attn, w_out, preferred_element_type=jnp.float32)
    normed = norm_rows(mixed, norm_gain).astype(jnp.bfloat16)
    logits = jnp.dot(normed, w_router, preferred_element_type=jnp.float32)
    expert_count = w_router.shape[1]
    picks = (routes[:, :, None] == jnp.arange(expert_count, dtype=jnp.int32)[None, None, :]).astype(jnp.float32)
    chosen = lax.optimization_barrier(jnp.sum(logits[:, None, :] * picks, axis=-1))
    route_weight = jax.nn.softmax(chosen, axis=-1)
    per_expert = lax.optimization_barrier(jnp.sum(route_weight[:, :, None] * picks, axis=1))
    expert_width = expert_w_gate.shape[1] // expert_count
    branch = jnp.zeros((tokens.shape[0], tokens.shape[1]), jnp.float32)
    for index in range(expert_count):
        low = index * expert_width
        gate_part = jnp.dot(normed, expert_w_gate[:, low:low + expert_width], preferred_element_type=jnp.float32)
        up_part = jnp.dot(normed, expert_w_up[:, low:low + expert_width], preferred_element_type=jnp.float32)
        hidden = (per_expert[:, index:index + 1] * jax.nn.silu(gate_part) * up_part).astype(jnp.bfloat16)
        branch = branch + jnp.dot(hidden, expert_w_down[low:low + expert_width], preferred_element_type=jnp.float32)
    dense_scale = jax.nn.sigmoid(jnp.dot(normed, dense_gate, preferred_element_type=jnp.float32))
    dense_gate_part = jnp.dot(normed, dense_w_gate, preferred_element_type=jnp.float32)
    dense_up_part = jnp.dot(normed, dense_w_up, preferred_element_type=jnp.float32)
    dense_hidden = (dense_scale[:, None] * jax.nn.silu(dense_gate_part) * dense_up_part).astype(jnp.bfloat16)
    branch = branch + jnp.dot(dense_hidden, dense_w_down, preferred_element_type=jnp.float32)
    final = residual_scale * normed.astype(jnp.float32) + branch
    return norm_rows(final, final_gain).astype(jnp.bfloat16)
```

```python
import functools

import jax
import jax.numpy as jnp
from jax import lax
from jax.experimental import pallas as pl
from jax.experimental.pallas import tpu as pltpu
from jax.sharding import PartitionSpec as P

norm_eps = 1e-05
residual_scale = 8.0**0.25
CORES = 2
LANES = 128
bf16 = jnp.bfloat16
f32 = jnp.float32
VM = pltpu.VMEM


def whole(space=VM):
    return pl.BlockSpec(memory_space=space)


def call(kernel, outs, ins, scratch=(), limit=None, cost=None):
    return pl.pallas_call(
        kernel,
        out_shape=outs,
        in_specs=ins,
        out_specs=jax.tree.map(lambda _: whole(), outs),
        scratch_shapes=list(scratch),
        cost_estimate=cost,
        compiler_params=pltpu.CompilerParams(vmem_limit_bytes=limit),
    )


def iota(shape, dim):
    return lax.broadcasted_iota(jnp.int32, shape, dim)


def nt(a, b):
    return lax.dot_general(a, b, (((1,), (1,)), ((), ())), preferred_element_type=f32)


def mm(a, b):
    return jnp.dot(a, b, preferred_element_type=f32)


def project(tok, tokp, wq, wk, wv, wf, pq, pk, pv, pf, wout, out, tok_out, wout_out):
    core = lax.rem(lax.axis_index("ep"), CORES)
    seqs = tok.shape[0]
    rows = seqs // CORES
    here = out.shape[1]
    r = iota((rows, seqs), 0)
    source = (r // here) * (CORES * here) + core * here + lax.rem(r, here)
    pick = (iota((rows, seqs), 1) == source).astype(f32).astype(bf16)
    own = mm(pick, tok[...]).astype(bf16)
    other = mm(pick, tokp[...]).astype(bf16)
    width = wq.shape[1]
    dest = rows // here
    for k, (w, p) in enumerate(((wq, pq), (wk, pk), (wv, pv))):
        term = mm(own, w[...]) + mm(other, p[...])
        out[:, :, k * width : (k + 1) * width] = term.reshape(dest, here, width).astype(bf16)
    heads = wf.shape[0]
    forget = nt(own, wf[...]) + nt(other, pf[...])
    high = forget.astype(bf16).astype(f32)
    low = forget - high
    pad = jnp.zeros((rows, LANES - 2 * heads), f32)
    both = jnp.concatenate([high, low, pad], axis=1)
    out[:, :, 3 * width : 3 * width + LANES] = both.reshape(dest, here, LANES).astype(bf16)
    feats = tok.shape[1]
    first = jnp.where(core == 0, own.astype(f32), other.astype(f32))
    second = jnp.where(core == 0, other.astype(f32), own.astype(f32))
    tok_out[...] = jnp.concatenate([first, second], axis=1)
    for z in range(dest):
        wout_out[z] = wout[:, z * LANES : (z + 1) * LANES]


def attention(got, gates, bias, lengths, keys, values, out):
    dest, here, _ = got.shape
    heads, places = gates.shape[1:]
    width = keys.shape[2]
    size = width // heads
    total = got[0].astype(f32)
    for z in range(1, dest):
        total = total + got[z].astype(f32)
    mine = iota((heads, width), 1) // size == iota((heads, width), 0)
    lane = iota((heads, LANES), 1)
    sub = iota((heads, LANES), 0)
    position = iota((heads, places), 1)
    scale = size**-0.5
    soft = []
    for j in range(here):
        row = total[j : j + 1]
        query = jnp.where(mine, row[:, :width].astype(bf16).astype(f32), 0.0)
        new_key = row[:, width : 2 * width].astype(bf16).astype(f32)
        tail = row[:, 3 * width : 3 * width + LANES]
        forget = jnp.sum(
            jnp.where((lane == sub) | (lane == sub + heads), tail, 0.0), axis=1, keepdims=True
        )
        x = forget + bias[...]
        log_gate = -(jnp.maximum(-x, 0.0) + jnp.log1p(jnp.exp(-jnp.abs(x))))
        gate = gates[j]
        length = lengths[j]
        last = jnp.sum(jnp.where(position == length - 1, gate, 0.0), axis=1, keepdims=True)
        own = jnp.sum(query * new_key, axis=1, keepdims=True) * scale
        scores = nt(query.astype(bf16), keys[j]) * scale + ((last + log_gate) - gate)
        scores = jnp.where(position < length, scores, -jnp.inf)
        top = jnp.maximum(jnp.max(scores, axis=1, keepdims=True), own)
        weights = jnp.exp(scores - top)
        weight_own = jnp.exp(own - top)
        sums = jnp.sum(weights, axis=1, keepdims=True) + weight_own
        soft.append(((weights / sums).astype(bf16), (weight_own / sums).astype(bf16).astype(f32)))
    rows = []
    for j in range(here):
        probs, prob_own = soft[j]
        new_value = total[j : j + 1, 2 * width : 3 * width].astype(bf16).astype(f32)
        mixed = mm(probs, values[j]) + prob_own * new_value
        rows.append(jnp.sum(jnp.where(mine, mixed, 0.0), axis=0, keepdims=True))
    attn = jnp.concatenate(rows, axis=0).astype(bf16)
    for z in range(dest):
        out[z] = attn


def out_project(got, wown, wpar, tok, out, wbuf):
    core = lax.rem(lax.axis_index("ep"), CORES)
    dest, here, width = got.shape
    part = wown.shape[1]
    for z in range(dest):
        wbuf[pl.ds(pl.multiple_of(z * CORES * part + core * part, part), part), :] = wown[z]
        wbuf[pl.ds(pl.multiple_of(z * CORES * part + (1 - core) * part, part), part), :] = wpar[z]
    attn = got[...].astype(f32).reshape(dest * here, width).astype(bf16)
    mixed = (mm(attn, wbuf[...]) + residual_scale * tok[...]).astype(bf16)
    for z in range(dest):
        out[z] = mixed


def feed_forward(
    xown, xpar, gain, small, routes, weg, weu, wdg, wdu, wed, wdd,
    keep, send, rest,
    xbuf,
):
    rank = lax.axis_index("ep")
    core = lax.rem(rank, CORES)
    chips, rows, lanes = xown.shape
    width = chips * lanes
    experts = small.shape[0] // 2
    for z in range(chips):
        at = slice(z * lanes, (z + 1) * lanes)
        xbuf[pl.ds(pl.multiple_of(core * rows, rows), rows), at] = xown[z]
        xbuf[pl.ds(pl.multiple_of((1 - core) * rows, rows), rows), at] = xpar[z]
    x = xbuf[...].astype(f32)
    center = jnp.sum(x, axis=1, keepdims=True) / width
    second = jnp.sum(x * x, axis=1, keepdims=True) / width
    normed = (x - center) * lax.rsqrt(second - center * center + norm_eps) * gain[...].astype(f32)
    normed = normed.astype(bf16)
    xbuf[...] = normed
    logits = nt(normed, small[...])
    slot = iota(logits.shape, 1)
    route0, route1 = routes[:, 0:1], routes[:, 1:2]
    logit0 = jnp.sum(jnp.where(slot == route0, logits, 0.0), axis=1, keepdims=True)
    logit1 = jnp.sum(jnp.where(slot == route1, logits, 0.0), axis=1, keepdims=True)
    peak = jnp.maximum(logit0, logit1)
    e0, e1 = jnp.exp(logit0 - peak), jnp.exp(logit1 - peak)
    expert = rank // (lax.axis_size("ep") // experts)
    weight = (jnp.where(route0 == expert, e0, 0.0) + jnp.where(route1 == expert, e1, 0.0)) / (e0 + e1)
    shut = jnp.sum(jnp.where(slot == experts, logits, 0.0), axis=1, keepdims=True)
    dense = 1.0 / (1.0 + jnp.exp(-shut))
    gate = mm(normed, weg[...])
    up = mm(normed, weu[...])
    hidden_e = (weight * (gate / (1.0 + jnp.exp(-gate))) * up).astype(bf16)
    gate = mm(normed, wdg[...])
    up = mm(normed, wdu[...])
    hidden_d = (dense * (gate / (1.0 + jnp.exp(-gate))) * up).astype(bf16)
    low = iota((rows, lanes), 1) < lanes // 2
    for z in range(chips):
        at = slice(z * lanes, (z + 1) * lanes)
        block = mm(hidden_e, wed[:, at]) + mm(hidden_d, wdd[:, at])
        above, below = block[:rows], block[rows:]
        zero = jnp.where(low, above, pltpu.roll(below, lanes // 2, 1))
        one = jnp.where(low, pltpu.roll(above, lanes // 2, 1), below)
        keep[z] = jnp.where(core == 0, zero, one)
        send[z] = jnp.where(core == 0, one, zero).astype(bf16)
    chip = rank // CORES
    own = xbuf[:, pl.ds(pl.multiple_of(chip * lanes, lanes), lanes)].astype(f32)
    above, below = own[:rows], own[rows:]
    zero = jnp.where(low, above, pltpu.roll(below, lanes // 2, 1))
    one = jnp.where(low, pltpu.roll(above, lanes // 2, 1), below)
    rest[...] = residual_scale * jnp.where(core == 0, zero, one)


def pair_sum(keep, got, out):
    out[...] = (keep[...] + got[...].astype(f32)).astype(bf16)


def gather_sums(got, rest, final, stats):
    chips, rows, lanes = got.shape
    total = rest[...]
    for z in range(chips):
        total = total + got[z].astype(f32)
    final[...] = total
    low = iota((rows, lanes), 1) < lanes // 2
    lane = iota((rows, lanes), 1)
    sub = iota((rows, lanes), 0)
    square = total * total
    line = jnp.zeros((1, lanes), f32)
    for k, v in enumerate(
        (
            jnp.where(low, total, 0.0),
            jnp.where(low, 0.0, total),
            jnp.where(low, square, 0.0),
            jnp.where(low, 0.0, square),
        )
    ):
        column = jnp.sum(v, axis=1, keepdims=True)
        line = line + jnp.sum(jnp.where(lane == sub + k * rows, column, 0.0), axis=0, keepdims=True)
    for d in range(stats.shape[0]):
        stats[d] = line


def finish(final, stats, gain, out):
    rows, lanes = final.shape
    ranks = stats.shape[0]
    line = stats[0]
    for d in range(1, ranks):
        line = line + stats[d]
    lane = iota((rows, lanes), 1)
    sub = iota((rows, lanes), 0)
    low = lane < lanes // 2
    width = ranks * (lanes // 2)
    columns = [
        jnp.sum(jnp.where(lane == sub + k * rows, line, 0.0), axis=1, keepdims=True) / width
        for k in range(4)
    ]
    center = jnp.where(low, columns[0], columns[1])
    second = jnp.where(low, columns[2], columns[3])
    unit = (final[...] - center) * lax.rsqrt(second - center * center + norm_eps)
    unit = (unit * gain[...].astype(f32)).astype(bf16)
    stacked = jnp.concatenate([unit[:, : lanes // 2], unit[:, lanes // 2 :]], axis=0)
    seqs = stacked.shape[0]
    here = seqs // ranks
    s = iota((seqs, seqs), 0)
    inside = lax.rem(s, CORES * here)
    source = (inside // here) * rows + (s // (CORES * here)) * here + lax.rem(inside, here)
    place = (iota((seqs, seqs), 1) == source).astype(f32).astype(bf16)
    out[...] = mm(place, stacked).astype(bf16)


def shards(
    tokens,
    w_query,
    w_key,
    w_value,
    w_forget,
    forget_bias,
    cache_keys,
    cache_values,
    cache_gates,
    lengths,
    w_out,
    norm_gain,
    w_router,
    routes,
    dense_gate,
    dense_w_gate,
    dense_w_up,
    dense_w_down,
    expert_w_gate,
    expert_w_up,
    expert_w_down,
    final_gain,
):
    ranks = lax.axis_size("ep")
    chips = ranks // CORES
    seqs, feats = tokens.shape
    here = seqs // ranks
    rows = seqs // CORES
    width = w_query.shape[1]
    heads = w_forget.shape[1]
    places = cache_keys.shape[1]
    model = w_out.shape[1]
    planes = [[CORES * z + c for z in range(chips)] for c in range(CORES)]
    pairs = [(i, i ^ 1) for i in range(ranks)]
    sds = jax.ShapeDtypeStruct

    def swap(a):
        return lax.ppermute(a, "ep", pairs)

    def exchange(a):
        return lax.all_to_all(
            a, "ep", split_axis=0, concat_axis=0, tiled=True, axis_index_groups=planes
        )

    wf = jnp.transpose(w_forget)
    sent = (tokens, w_query, w_key, w_value, wf)
    tokp, pq, pk, pv, pf = (swap(a) for a in sent)
    terms, tok, wcols = call(
        project,
        (
            sds((chips, here, 3 * width + LANES), bf16),
            sds((rows, LANES), f32),
            sds((chips, w_out.shape[0], LANES), bf16),
        ),
        [whole()] * 11,
        limit=8 << 20,
    )(tokens, tokp, w_query, w_key, w_value, wf, pq, pk, pv, pf, w_out)
    sums = exchange(terms)
    wown = exchange(wcols)
    attn = call(
        attention,
        sds((chips, here, width), bf16),
        [whole(), whole(), whole(), whole(pltpu.SMEM), whole(), whole()],
        limit=14 << 20,
    )(
        sums,
        jnp.transpose(cache_gates, (0, 2, 1)),
        forget_bias.reshape(heads, 1),
        lengths,
        cache_keys,
        cache_values,
    )
    attn_all = exchange(attn)
    wpar = swap(wown)
    mixed = call(
        out_project,
        sds((chips, rows, LANES), bf16),
        [whole()] * 4,
        [VM((width, LANES), bf16)],
        limit=4 << 20,
    )(attn_all, wown, wpar, tok)
    xown = exchange(mixed)
    xpar = swap(xown)
    experts = w_router.shape[1]
    small = jnp.concatenate(
        [
            jnp.transpose(w_router),
            dense_gate[None],
            jnp.zeros((experts - 1, model), bf16),
        ]
    )
    routes_planes = (
        routes.reshape(chips, CORES, here, routes.shape[1])
        .transpose(1, 0, 2, 3)
        .reshape(seqs, routes.shape[1])
    )
    weights = (expert_w_gate, expert_w_up, dense_w_gate, dense_w_up, expert_w_down, dense_w_down)
    keep, send, rest = call(
        feed_forward,
        (
            sds((chips, rows, LANES), f32),
            sds((chips, rows, LANES), bf16),
            sds((rows, LANES), f32),
        ),
        [whole()] * 11,
        [VM((seqs, model), bf16)],
        limit=18 << 20,
    )(xown, xpar, norm_gain[None], small, routes_planes, *weights)
    part = call(pair_sum, sds((chips, rows, LANES), bf16), [whole()] * 2, limit=4 << 20)(
        keep, swap(send)
    )
    final, stats = call(
        gather_sums,
        (sds((rows, LANES), f32), sds((ranks, 1, LANES), f32)),
        [whole()] * 2,
        limit=4 << 20,
    )(exchange(part), rest)
    stats = lax.all_to_all(stats, "ep", split_axis=0, concat_axis=0, tiled=True)
    gain2 = jnp.concatenate([final_gain, final_gain])[None]
    return call(finish, sds((seqs, feats), bf16), [whole()] * 3, limit=4 << 20)(
        final, stats, gain2
    )


def solution(mesh):
    placed = (
        P("grp", "ep"),
        P("ep", None),
        P("ep", None),
        P("ep", None),
        P("ep", None),
        P(),
        P(("grp", "ep"), None, None),
        P(("grp", "ep"), None, None),
        P(("grp", "ep"), None, None),
        P(("grp", "ep")),
        P("ep", None),
        P(),
        P(),
        P("grp", None),
        P(),
        P(None, "ep"),
        P(None, "ep"),
        P("ep", None),
        P(None, "ep"),
        P(None, "ep"),
        P("ep", None),
        P("ep"),
    )
    return jax.shard_map(
        shards, mesh=mesh, in_specs=placed, out_specs=P("grp", "ep"), check_vma=False
    )
```

```python
import jax
import jax.numpy as jnp
from jax import lax
from jax.experimental import pallas as pl
from jax.experimental.pallas import tpu as pltpu
from jax.sharding import PartitionSpec as P


norm_eps = 1e-05
residual_scale = 8.0**0.25
CORES = 2
LANES = 128
bf16 = jnp.bfloat16
f32 = jnp.float32
VM = pltpu.VMEM
HBM = pltpu.HBM


def whole(space=VM):
    return pl.BlockSpec(memory_space=space)


def call(kernel, outs, ins, scratch=(), limit=None):
    return pl.pallas_call(
        kernel,
        out_shape=outs,
        in_specs=ins,
        out_specs=jax.tree.map(lambda _: whole(), outs),
        scratch_shapes=list(scratch),
        compiler_params=pltpu.CompilerParams(vmem_limit_bytes=limit),
    )


def iota(shape, dim):
    return lax.broadcasted_iota(jnp.int32, shape, dim)


def nt(a, b):
    return lax.dot_general(a, b, (((1,), (1,)), ((), ())), preferred_element_type=f32)


def mm(a, b):
    return jnp.dot(a, b, preferred_element_type=f32)


def project(
    tokp, pq, pk, pv, pf, tok_hbm, wq_hbm, wk_hbm, wv_hbm, wf_hbm, wout_hbm,
    out, tok_out, tok, wq, wk, wv, wf, wout, pairs, sems,
):
    copies = [
        pltpu.make_async_copy(src, dst, sems.at[k])
        for k, (src, dst) in enumerate(
            (
                (tok_hbm, tok),
                (wq_hbm, wq),
                (wk_hbm, wk),
                (wv_hbm, wv),
                (wf_hbm, wf),
                (wout_hbm, wout),
            )
        )
    ]
    for c in copies:
        c.start()
    core = lax.rem(lax.axis_index("ep"), CORES)
    seqs = tok.shape[0]
    rows = seqs // CORES
    here = out.shape[1]
    r = iota((rows, seqs), 0)
    source = (r // here) * (CORES * here) + core * here + lax.rem(r, here)
    pick = (iota((rows, seqs), 1) == source).astype(f32).astype(bf16)
    other = mm(pick, tokp[...]).astype(bf16)
    copies[0].wait()
    own = mm(pick, tok[...]).astype(bf16)
    width = wq.shape[1]
    dest = rows // here
    for k, (w, p) in enumerate(((wq, pq), (wk, pk), (wv, pv))):
        copies[k + 1].wait()
        term = mm(own, w[...]) + mm(other, p[...])
        out[:, :, k * width : (k + 1) * width] = term.reshape(dest, here, width).astype(bf16)
    heads = wf.shape[0]
    copies[4].wait()
    forget = nt(own, wf[...]) + nt(other, pf[...])
    high = forget.astype(bf16).astype(f32)
    low = forget - high
    pad = jnp.zeros((rows, LANES - 2 * heads), f32)
    both = jnp.concatenate([high, low, pad], axis=1)
    out[:, :, 3 * width : 3 * width + LANES] = both.reshape(dest, here, LANES).astype(bf16)
    first = jnp.where(core == 0, own.astype(f32), other.astype(f32))
    second = jnp.where(core == 0, other.astype(f32), own.astype(f32))
    tok_out[...] = jnp.concatenate([first, second], axis=1)
    copies[5].wait()
    steps = pairs.shape[0]
    pairs[...] = wout[...].reshape(pairs.shape)
    base = 3 * width + LANES
    for z in range(dest):
        for t in range(steps):
            out[z, :, base + t * LANES : base + (t + 1) * LANES] = pairs[
                t, :, z * LANES : (z + 1) * LANES
            ]


def unpack_columns(got, out):
    dest, here, _ = got.shape
    steps = out.shape[1] // here
    base = got.shape[2] - steps * LANES
    for z in range(dest):
        out[z] = jnp.concatenate(
            [
                got[z, :, base + t * LANES : base + (t + 1) * LANES].astype(f32)
                for t in range(steps)
            ],
            axis=0,
        ).astype(bf16)


def load_cache(lengths, keys_hbm, gates_hbm, keys, bias, gates, sems):
    copies = [
        pltpu.make_async_copy(gates_hbm, gates, sems.at[0]),
        pltpu.make_async_copy(keys_hbm.at[0], keys, sems.at[1]),
    ]
    for c in copies:
        c.start()
    copies[0].wait()
    for j in range(gates.shape[0]):
        gate = gates[j]
        length = lengths[j]
        position = iota(gate.shape, 1)
        last = jnp.sum(jnp.where(position == length - 1, gate, 0.0), axis=1, keepdims=True)
        bias[j] = jnp.where(position < length, last - gate, -jnp.inf)
    copies[1].wait()


def load_all(*refs):
    count = len(refs) // 2
    sems = refs[-1]
    copies = [
        pltpu.make_async_copy(refs[k], refs[count + k], sems.at[k]) for k in range(count)
    ]
    for c in copies:
        c.start()
    for c in copies:
        c.wait()


def attention(
    got, bias, forget_bias, first, keys_hbm, values_hbm, out, keys, values, sems
):
    dest, here, _ = got.shape
    heads = bias.shape[1]
    width = first.shape[1]
    kcopy = [
        pltpu.make_async_copy(keys_hbm.at[j], keys.at[j - 1], sems.at[0, j]) for j in range(1, here)
    ]
    vcopy = [
        pltpu.make_async_copy(values_hbm.at[j], values.at[j], sems.at[1, j]) for j in range(here)
    ]
    for c in kcopy + vcopy:
        c.start()
    size = width // heads
    used = 3 * width + LANES
    total = got[0, :, :used].astype(f32)
    for z in range(1, dest):
        total = total + got[z, :, :used].astype(f32)
    mine = iota((heads, width), 1) // size == iota((heads, width), 0)
    lane = iota((heads, LANES), 1)
    sub = iota((heads, LANES), 0)
    scale = size**-0.5
    added = jnp.sum(jnp.where(lane == sub, forget_bias[...], 0.0), axis=1, keepdims=True)
    soft = []
    for j in range(here):
        row = total[j : j + 1]
        query = jnp.where(mine, row[:, :width].astype(bf16).astype(f32), 0.0)
        new_key = row[:, width : 2 * width].astype(bf16).astype(f32)
        tail = row[:, 3 * width : 3 * width + LANES]
        forget = jnp.sum(
            jnp.where((lane == sub) | (lane == sub + heads), tail, 0.0), axis=1, keepdims=True
        )
        x = forget + added
        log_gate = -(jnp.maximum(-x, 0.0) + jnp.log1p(jnp.exp(-jnp.abs(x))))
        own = jnp.sum(query * new_key, axis=1, keepdims=True) * scale
        if j > 0:
            kcopy[j - 1].wait()
        keys_here = first[...] if j == 0 else keys[j - 1]
        scores = nt(query.astype(bf16), keys_here) * scale + (bias[j] + log_gate)
        top = jnp.maximum(jnp.max(scores, axis=1, keepdims=True), own)
        weights = jnp.exp(scores - top)
        weight_own = jnp.exp(own - top)
        sums = jnp.sum(weights, axis=1, keepdims=True) + weight_own
        soft.append(((weights / sums).astype(bf16), (weight_own / sums).astype(bf16).astype(f32)))
    rows = []
    for j in range(here):
        probs, prob_own = soft[j]
        new_value = total[j : j + 1, 2 * width : 3 * width].astype(bf16).astype(f32)
        vcopy[j].wait()
        mixed = mm(probs, values[j]) + prob_own * new_value
        rows.append(jnp.sum(jnp.where(mine, mixed, 0.0), axis=0, keepdims=True))
    attn = jnp.concatenate(rows, axis=0).astype(bf16)
    for z in range(dest):
        out[z] = attn


def out_project(got, wown, wpar, tok, out, wbuf):
    core = lax.rem(lax.axis_index("ep"), CORES)
    dest, here, width = got.shape
    part = wown.shape[1]
    for z in range(dest):
        wbuf[pl.ds(pl.multiple_of(z * CORES * part + core * part, part), part), :] = wown[z]
        wbuf[pl.ds(pl.multiple_of(z * CORES * part + (1 - core) * part, part), part), :] = wpar[z]
    attn = got[...].astype(f32).reshape(dest * here, width).astype(bf16)
    mixed = (mm(attn, wbuf[...]) + residual_scale * tok[...]).astype(bf16)
    for z in range(dest):
        out[z] = mixed


def feed_forward(
    xown, xpar, gain, shutter, router, routes, weg, wdg,
    weu_hbm, wdu_hbm, wed_hbm, wdd_hbm,
    keep, send, rest,
    xbuf, weu, wdu, wed, wdd, sems,
):
    rank = lax.axis_index("ep")
    ranks = lax.axis_size("ep")
    core = lax.rem(rank, CORES)
    copies = [
        pltpu.make_async_copy(src, dst, sems.at[k])
        for k, (src, dst) in enumerate(
            ((weu_hbm, weu), (wdu_hbm, wdu), (wed_hbm, wed), (wdd_hbm, wdd))
        )
    ]
    for c in copies:
        c.start()
    chips, rows, lanes = xown.shape
    width = chips * lanes
    seqs = CORES * rows
    here = seqs // ranks
    experts = router.shape[0]
    low = iota((rows, lanes), 1) < lanes // 2
    chip = rank // CORES
    for half, ref in ((core, xown), (1 - core, xpar)):
        x = ref[...].astype(f32)
        ones = jnp.sum(x, axis=0)
        squares = jnp.sum(x * x, axis=0)
        center = jnp.sum(ones, axis=1, keepdims=True) / width
        second = jnp.sum(squares, axis=1, keepdims=True) / width
        factor = lax.rsqrt(second - center * center + norm_eps)
        for z in range(chips):
            block = (x[z] - center) * factor * gain[z : z + 1, :].astype(f32)
            xbuf[pl.ds(pl.multiple_of(half * rows, rows), rows), z * lanes : (z + 1) * lanes] = (
                block.astype(bf16)
            )
    normed = xbuf[...]
    logits = nt(normed, router[...])
    slot = iota(logits.shape, 1)
    r = iota((seqs, seqs), 0)
    inside = lax.rem(r, rows)
    source = (inside // here) * (CORES * here) + (r // rows) * here + lax.rem(inside, here)
    same = iota((seqs, seqs), 1) == source
    route0 = jnp.sum(jnp.where(same, routes[0:1, :], 0), axis=1, keepdims=True)
    route1 = jnp.sum(jnp.where(same, routes[1:2, :], 0), axis=1, keepdims=True)
    logit0 = jnp.sum(jnp.where(slot == route0, logits, 0.0), axis=1, keepdims=True)
    logit1 = jnp.sum(jnp.where(slot == route1, logits, 0.0), axis=1, keepdims=True)
    peak = jnp.maximum(logit0, logit1)
    e0, e1 = jnp.exp(logit0 - peak), jnp.exp(logit1 - peak)
    expert = rank // (ranks // experts)
    weight = (jnp.where(route0 == expert, e0, 0.0) + jnp.where(route1 == expert, e1, 0.0)) / (e0 + e1)
    shut = jnp.zeros((seqs, lanes), f32)
    for z in range(chips):
        block = xbuf[:, z * lanes : (z + 1) * lanes].astype(f32)
        shut = shut + block * shutter[z : z + 1, :].astype(f32)
    shut = jnp.sum(shut, axis=1, keepdims=True)
    dense = 1.0 / (1.0 + jnp.exp(-shut))
    gate_e = mm(normed, weg[...])
    gate_d = mm(normed, wdg[...])
    copies[0].wait()
    up_e = mm(normed, weu[...])
    hidden_e = (weight * (gate_e / (1.0 + jnp.exp(-gate_e))) * up_e).astype(bf16)
    copies[1].wait()
    up_d = mm(normed, wdu[...])
    hidden_d = (dense * (gate_d / (1.0 + jnp.exp(-gate_d))) * up_d).astype(bf16)
    copies[2].wait()
    copies[3].wait()
    for z in range(chips):
        at = slice(z * lanes, (z + 1) * lanes)
        block = mm(hidden_e, wed[:, at]) + mm(hidden_d, wdd[:, at])
        above, below = block[:rows], block[rows:]
        zero = jnp.where(low, above, pltpu.roll(below, lanes // 2, 1))
        one = jnp.where(low, pltpu.roll(above, lanes // 2, 1), below)
        keep[z] = jnp.where(core == 0, zero, one)
        send[z] = jnp.where(core == 0, one, zero).astype(bf16)
    own = xbuf[:, pl.ds(pl.multiple_of(chip * lanes, lanes), lanes)].astype(f32)
    above, below = own[:rows], own[rows:]
    zero = jnp.where(low, above, pltpu.roll(below, lanes // 2, 1))
    one = jnp.where(low, pltpu.roll(above, lanes // 2, 1), below)
    rest[...] = residual_scale * jnp.where(core == 0, zero, one)


def pair_sum(keep, got, out):
    out[...] = (keep[...] + got[...].astype(f32)).astype(bf16)


def gather_sums(got, rest, final, stats):
    chips, rows, lanes = got.shape
    total = rest[...]
    for z in range(chips):
        total = total + got[z].astype(f32)
    final[...] = total
    low = iota((rows, lanes), 1) < lanes // 2
    lane = iota((rows, lanes), 1)
    sub = iota((rows, lanes), 0)
    square = total * total
    line = jnp.zeros((1, lanes), f32)
    for k, v in enumerate(
        (
            jnp.where(low, total, 0.0),
            jnp.where(low, 0.0, total),
            jnp.where(low, square, 0.0),
            jnp.where(low, 0.0, square),
        )
    ):
        column = jnp.sum(v, axis=1, keepdims=True)
        line = line + jnp.sum(jnp.where(lane == sub + k * rows, column, 0.0), axis=0, keepdims=True)
    for d in range(stats.shape[0]):
        stats[d] = line


def finish(final, stats, gain, out):
    rows, lanes = final.shape
    ranks = stats.shape[0]
    line = stats[0]
    for d in range(1, ranks):
        line = line + stats[d]
    lane = iota((rows, lanes), 1)
    sub = iota((rows, lanes), 0)
    low = lane < lanes // 2
    width = ranks * (lanes // 2)
    columns = [
        jnp.sum(jnp.where(lane == sub + k * rows, line, 0.0), axis=1, keepdims=True) / width
        for k in range(4)
    ]
    center = jnp.where(low, columns[0], columns[1])
    second = jnp.where(low, columns[2], columns[3])
    unit = (final[...] - center) * lax.rsqrt(second - center * center + norm_eps)
    stacked = jnp.concatenate([unit[:, : lanes // 2], unit[:, lanes // 2 :]], axis=0)
    stacked = (stacked * gain[...].reshape(1, lanes // 2).astype(f32)).astype(bf16)
    seqs = stacked.shape[0]
    here = seqs // ranks
    s = iota((seqs, seqs), 0)
    inside = lax.rem(s, CORES * here)
    source = (inside // here) * rows + (s // (CORES * here)) * here + lax.rem(inside, here)
    place = (iota((seqs, seqs), 1) == source).astype(f32).astype(bf16)
    out[...] = mm(place, stacked).astype(bf16)


def shards(
    tokens,
    w_query,
    w_key,
    w_value,
    w_forget,
    forget_bias,
    cache_keys,
    cache_values,
    cache_gates,
    lengths,
    w_out,
    norm_gain,
    w_router,
    routes,
    dense_gate,
    dense_w_gate,
    dense_w_up,
    dense_w_down,
    expert_w_gate,
    expert_w_up,
    expert_w_down,
    final_gain,
):
    ranks = lax.axis_size("ep")
    chips = ranks // CORES
    seqs, feats = tokens.shape
    here = seqs // ranks
    rows = seqs // CORES
    width = w_query.shape[1]
    heads = w_forget.shape[1]
    places = cache_keys.shape[1]
    model = w_out.shape[1]
    planes = [[CORES * z + c for z in range(chips)] for c in range(CORES)]
    pairs = [(i, i ^ 1) for i in range(ranks)]
    sds = jax.ShapeDtypeStruct

    def far(arrays):
        return tuple(pltpu.with_memory_space_constraint(a, HBM) for a in arrays)

    def swap(a):
        return lax.ppermute(a, "ep", pairs)

    def exchange(a):
        return lax.all_to_all(
            a, "ep", split_axis=0, concat_axis=0, tiled=True, axis_index_groups=planes
        )

    dma = pltpu.SemaphoreType.DMA
    wf = jnp.transpose(w_forget)
    sent = (tokens, w_query, w_key, w_value, wf)
    arrived = tuple(swap(a) for a in sent)
    terms, tok = call(
        project,
        (
            sds((chips, here, 3 * width + LANES + w_out.shape[0] // here * LANES), bf16),
            sds((rows, LANES), f32),
        ),
        [whole()] * 5 + [whole(HBM)] * 6,
        [VM(a.shape, bf16) for a in (*sent, w_out)]
        + [VM((w_out.shape[0] // here, here, model), bf16), dma((6,))],
        limit=8 << 20,
    )(*arrived, *far((*sent, w_out)))
    sums = exchange(terms)
    wown = call(
        unpack_columns,
        sds((chips, w_out.shape[0], LANES), bf16),
        [whole()],
        limit=4 << 20,
    )(sums)
    gates = jnp.transpose(cache_gates, (0, 2, 1))
    far_keys, far_values, gates = far((cache_keys, cache_values, gates))
    first, bias = call(
        load_cache,
        (VM(cache_keys.shape[1:], bf16), VM(gates.shape, f32)),
        [whole(pltpu.SMEM)] + [whole(HBM)] * 2,
        [VM(gates.shape, f32), dma((2,))],
        limit=4 << 20,
    )(lengths, far_keys, gates)
    forget_row = jnp.pad(forget_bias, (0, LANES - heads))[None]
    attn = call(
        attention,
        sds((chips, here, width), bf16),
        [whole()] * 4 + [whole(HBM)] * 2,
        [
            VM((here - 1, places, width), bf16),
            VM((here, places, width), bf16),
            dma((2, here)),
        ],
        limit=14 << 20,
    )(sums, bias, forget_row, first, far_keys, far_values)
    attn_all = exchange(attn)
    wpar = swap(wown)
    mixed = call(
        out_project,
        sds((chips, rows, LANES), bf16),
        [whole()] * 4,
        [VM((width, LANES), bf16)],
        limit=4 << 20,
    )(attn_all, wown, wpar, tok)
    xown = exchange(mixed)
    xpar = swap(xown)
    weights = far(
        (expert_w_gate, dense_w_gate, expert_w_up, dense_w_up, expert_w_down, dense_w_down)
    )
    first = call(
        load_all,
        tuple(VM(w.shape, bf16) for w in weights[:2]),
        [whole(HBM)] * 2,
        [dma((2,))],
        limit=4 << 20,
    )(*weights[:2])
    keep, send, rest = call(
        feed_forward,
        (
            sds((chips, rows, LANES), f32),
            sds((chips, rows, LANES), bf16),
            sds((rows, LANES), f32),
        ),
        [whole()] * 8 + [whole(HBM)] * 4,
        [VM((seqs, model), bf16)] + [VM(w.shape, bf16) for w in weights[2:]] + [dma((4,))],
        limit=18 << 20,
    )(
        xown,
        xpar,
        norm_gain.reshape(chips, LANES),
        dense_gate.reshape(chips, LANES),
        jnp.transpose(w_router),
        jnp.transpose(routes),
        *first,
        *weights[2:],
    )
    part = call(pair_sum, sds((chips, rows, LANES), bf16), [whole()] * 2, limit=4 << 20)(
        keep, swap(send)
    )
    final, stats = call(
        gather_sums,
        (sds((rows, LANES), f32), sds((ranks, 1, LANES), f32)),
        [whole()] * 2,
        limit=4 << 20,
    )(exchange(part), rest)
    stats = lax.all_to_all(stats, "ep", split_axis=0, concat_axis=0, tiled=True)
    return call(finish, sds((seqs, feats), bf16), [whole()] * 3, limit=4 << 20)(
        final, stats, final_gain
    )


def solution(mesh):
    placed = (
        P("grp", "ep"),
        P("ep", None),
        P("ep", None),
        P("ep", None),
        P("ep", None),
        P(),
        P(("grp", "ep"), None, None),
        P(("grp", "ep"), None, None),
        P(("grp", "ep"), None, None),
        P(("grp", "ep")),
        P("ep", None),
        P(),
        P(),
        P("grp", None),
        P(),
        P(None, "ep"),
        P(None, "ep"),
        P("ep", None),
        P(None, "ep"),
        P(None, "ep"),
        P("ep", None),
        P("ep"),
    )

    return jax.shard_map(
        shards, mesh=mesh, in_specs=placed, out_specs=P("grp", "ep"), check_vma=False
    )
```

```python
import jax
import jax.numpy as jnp
from jax import lax
from jax.experimental import pallas as pl
from jax.experimental.pallas import tpu as pltpu
from jax.sharding import PartitionSpec as P


norm_eps = 1e-05
residual_scale = 8.0**0.25
CORES = 2
LANES = 128
bf16 = jnp.bfloat16
f32 = jnp.float32
VM = pltpu.VMEM
HBM = pltpu.HBM


def whole(space=VM):
    return pl.BlockSpec(memory_space=space)


def call(kernel, outs, ins, scratch=(), limit=None):
    return pl.pallas_call(
        kernel,
        out_shape=outs,
        in_specs=ins,
        out_specs=jax.tree.map(lambda _: whole(), outs),
        scratch_shapes=list(scratch),
        compiler_params=pltpu.CompilerParams(vmem_limit_bytes=limit),
    )


def iota(shape, dim):
    return lax.broadcasted_iota(jnp.int32, shape, dim)


def nt(a, b):
    return lax.dot_general(a, b, (((1,), (1,)), ((), ())), preferred_element_type=f32)


def mm(a, b):
    return jnp.dot(a, b, preferred_element_type=f32)


def plane_rows(rows, seqs, here):
    core = lax.rem(lax.axis_index("ep"), CORES)
    r = iota((rows, seqs), 0)
    source = (r // here) * (CORES * here) + core * here + lax.rem(r, here)
    return (iota((rows, seqs), 1) == source).astype(f32).astype(bf16)


def project_own(
    tok_hbm, wq_hbm, wk_hbm, wv_hbm, wf_hbm, wout_hbm,
    partial, own_out, pairs, tok, wq, wk, wv, wf, wout, sems,
):
    copies = [
        pltpu.make_async_copy(src, dst, sems.at[k])
        for k, (src, dst) in enumerate(
            (
                (tok_hbm, tok),
                (wq_hbm, wq),
                (wk_hbm, wk),
                (wv_hbm, wv),
                (wf_hbm, wf),
                (wout_hbm, wout),
            )
        )
    ]
    for c in copies:
        c.start()
    rows = own_out.shape[0]
    pick = plane_rows(rows, tok.shape[0], pairs.shape[1])
    for c in copies:
        c.wait()
    own = mm(pick, tok[...]).astype(bf16)
    own_out[...] = own
    width = wq.shape[1]
    for k, w in enumerate((wq, wk, wv)):
        partial[:, k * width : (k + 1) * width] = mm(own, w[...])
    forget = nt(own, wf[...])
    heads = wf.shape[0]
    pad = jnp.zeros((rows, LANES - 2 * heads), f32)
    partial[:, 3 * width :] = jnp.concatenate([forget, forget, pad], axis=1)
    pairs[...] = wout[...].reshape(pairs.shape)


def project_pair(partial, own, pairs, tokp, pq, pk, pv, pf, out, tok_out):
    core = lax.rem(lax.axis_index("ep"), CORES)
    dest, here, _ = out.shape
    rows = own.shape[0]
    other = mm(plane_rows(rows, tokp.shape[0], here), tokp[...]).astype(bf16)
    width = pq.shape[1]
    for k, p in enumerate((pq, pk, pv)):
        at = slice(k * width, (k + 1) * width)
        term = partial[:, at] + mm(other, p[...])
        out[:, :, at] = term.reshape(dest, here, width).astype(bf16)
    heads = pf.shape[0]
    forget = nt(other, pf[...])
    pad = jnp.zeros((rows, LANES - 2 * heads), f32)
    both = partial[:, 3 * width :] + jnp.concatenate([forget, forget, pad], axis=1)
    high = both.astype(bf16).astype(f32)
    both = jnp.where(iota(both.shape, 1) < heads, high, both - high)
    out[:, :, 3 * width : 3 * width + LANES] = both.reshape(dest, here, LANES).astype(bf16)
    mine = own[...].astype(f32)
    other = other.astype(f32)
    first = jnp.where(core == 0, mine, other)
    second = jnp.where(core == 0, other, mine)
    tok_out[...] = jnp.concatenate([first, second], axis=1)
    base = 3 * width + LANES
    for z in range(dest):
        for t in range(pairs.shape[0]):
            out[z, :, base + t * LANES : base + (t + 1) * LANES] = pairs[
                t, :, z * LANES : (z + 1) * LANES
            ]


def unpack_columns(got, out):
    dest, here, _ = got.shape
    steps = out.shape[1] // here
    base = got.shape[2] - steps * LANES
    for z in range(dest):
        out[z] = jnp.concatenate(
            [
                got[z, :, base + t * LANES : base + (t + 1) * LANES].astype(f32)
                for t in range(steps)
            ],
            axis=0,
        ).astype(bf16)


def load_all(*refs):
    count = len(refs) // 2
    sems = refs[-1]
    copies = [
        pltpu.make_async_copy(refs[k], refs[count + k], sems.at[k]) for k in range(count)
    ]
    for c in copies:
        c.start()
    for c in copies:
        c.wait()


def attention(
    got, forget_bias, lengths_hbm, gates_hbm, keys_hbm, values_hbm, out,
    lengths, gates, keys, values, sems,
):
    dest, here, _ = got.shape
    heads, places = gates.shape[1:]
    width = keys.shape[2]
    small = [
        pltpu.make_async_copy(lengths_hbm, lengths, sems.at[2, 0]),
        pltpu.make_async_copy(gates_hbm, gates, sems.at[2, 1]),
    ]
    kcopy = [pltpu.make_async_copy(keys_hbm.at[j], keys.at[j], sems.at[0, j]) for j in range(here)]
    vcopy = [
        pltpu.make_async_copy(values_hbm.at[j], values.at[j], sems.at[1, j]) for j in range(here)
    ]
    for c in small + kcopy + vcopy:
        c.start()
    size = width // heads
    used = 3 * width + LANES
    total = got[0, :, :used].astype(f32)
    for z in range(1, dest):
        total = total + got[z, :, :used].astype(f32)
    mine = iota((heads, width), 1) // size == iota((heads, width), 0)
    lane = iota((heads, LANES), 1)
    sub = iota((heads, LANES), 0)
    scale = size**-0.5
    position = iota((heads, places), 1)
    added = jnp.sum(
        jnp.where(
            iota((heads, heads), 1) == iota((heads, heads), 0), forget_bias[...], 0.0
        ),
        axis=1,
        keepdims=True,
    )
    for c in small:
        c.wait()
    soft = []
    for j in range(here):
        row = total[j : j + 1]
        query = jnp.where(mine, row[:, :width].astype(bf16).astype(f32), 0.0)
        new_key = row[:, width : 2 * width].astype(bf16).astype(f32)
        tail = row[:, 3 * width : 3 * width + LANES]
        forget = jnp.sum(
            jnp.where((lane == sub) | (lane == sub + heads), tail, 0.0), axis=1, keepdims=True
        )
        x = forget + added
        log_gate = -(jnp.maximum(-x, 0.0) + jnp.log1p(jnp.exp(-jnp.abs(x))))
        own = jnp.sum(query * new_key, axis=1, keepdims=True) * scale
        gate = gates[j]
        length = lengths[j]
        last = jnp.sum(jnp.where(position == length - 1, gate, 0.0), axis=1, keepdims=True)
        bias = jnp.where(position < length, (last + log_gate) - gate, -jnp.inf)
        kcopy[j].wait()
        scores = nt(query.astype(bf16), keys[j]) * scale + bias
        top = jnp.maximum(jnp.max(scores, axis=1, keepdims=True), own)
        weights = jnp.exp(scores - top)
        weight_own = jnp.exp(own - top)
        sums = jnp.sum(weights, axis=1, keepdims=True) + weight_own
        soft.append(((weights / sums).astype(bf16), (weight_own / sums).astype(bf16).astype(f32)))
    rows = []
    for j in range(here):
        probs, prob_own = soft[j]
        vcopy[j].wait()
        new_value = total[j : j + 1, 2 * width : 3 * width].astype(bf16).astype(f32)
        mixed = mm(probs, values[j]) + prob_own * new_value
        rows.append(jnp.sum(jnp.where(mine, mixed, 0.0), axis=0, keepdims=True))
    attn = jnp.concatenate(rows, axis=0).astype(bf16)
    for z in range(dest):
        out[z] = attn


def out_project(got, wown, wpar, tok, out, wbuf):
    core = lax.rem(lax.axis_index("ep"), CORES)
    dest, here, width = got.shape
    part = wown.shape[1]
    for z in range(dest):
        wbuf[pl.ds(pl.multiple_of(z * CORES * part + core * part, part), part), :] = wown[z]
        wbuf[pl.ds(pl.multiple_of(z * CORES * part + (1 - core) * part, part), part), :] = wpar[z]
    attn = got[...].astype(f32).reshape(dest * here, width).astype(bf16)
    mixed = (mm(attn, wbuf[...]) + residual_scale * tok[...]).astype(bf16)
    for z in range(dest):
        out[z] = mixed


def feed_forward(
    xown, xpar, gain, shutter, router, routes, weg, wdg, weu, wdu,
    wed_hbm, wdd_hbm,
    keep, send, rest,
    xbuf, wed, wdd, sems,
):
    rank = lax.axis_index("ep")
    ranks = lax.axis_size("ep")
    core = lax.rem(rank, CORES)
    copies = [
        pltpu.make_async_copy(src, dst, sems.at[k])
        for k, (src, dst) in enumerate(
            ((wed_hbm, wed), (wdd_hbm, wdd))
        )
    ]
    for c in copies:
        c.start()
    chips, rows, lanes = xown.shape
    width = chips * lanes
    seqs = CORES * rows
    here = seqs // ranks
    experts = router.shape[0]
    low = iota((rows, lanes), 1) < lanes // 2
    chip = rank // CORES
    for half, ref in ((core, xown), (1 - core, xpar)):
        x = ref[...].astype(f32)
        ones = jnp.sum(x, axis=0)
        squares = jnp.sum(x * x, axis=0)
        center = jnp.sum(ones, axis=1, keepdims=True) / width
        second = jnp.sum(squares, axis=1, keepdims=True) / width
        factor = lax.rsqrt(second - center * center + norm_eps)
        for z in range(chips):
            block = (x[z] - center) * factor * gain[z : z + 1, :].astype(f32)
            xbuf[pl.ds(pl.multiple_of(half * rows, rows), rows), z * lanes : (z + 1) * lanes] = (
                block.astype(bf16)
            )
    normed = xbuf[...]
    logits = nt(normed, router[...])
    slot = iota(logits.shape, 1)
    r = iota((seqs, seqs), 0)
    inside = lax.rem(r, rows)
    source = (inside // here) * (CORES * here) + (r // rows) * here + lax.rem(inside, here)
    same = iota((seqs, seqs), 1) == source
    route0 = jnp.sum(jnp.where(same, routes[0:1, :], 0), axis=1, keepdims=True)
    route1 = jnp.sum(jnp.where(same, routes[1:2, :], 0), axis=1, keepdims=True)
    logit0 = jnp.sum(jnp.where(slot == route0, logits, 0.0), axis=1, keepdims=True)
    logit1 = jnp.sum(jnp.where(slot == route1, logits, 0.0), axis=1, keepdims=True)
    peak = jnp.maximum(logit0, logit1)
    e0, e1 = jnp.exp(logit0 - peak), jnp.exp(logit1 - peak)
    expert = rank // (ranks // experts)
    weight = (jnp.where(route0 == expert, e0, 0.0) + jnp.where(route1 == expert, e1, 0.0)) / (e0 + e1)
    shut = jnp.zeros((seqs, lanes), f32)
    for z in range(chips):
        block = xbuf[:, z * lanes : (z + 1) * lanes].astype(f32)
        shut = shut + block * shutter[z : z + 1, :].astype(f32)
    shut = jnp.sum(shut, axis=1, keepdims=True)
    dense = 1.0 / (1.0 + jnp.exp(-shut))
    gate_e = mm(normed, weg[...])
    gate_d = mm(normed, wdg[...])
    up_e = mm(normed, weu[...])
    hidden_e = (weight * (gate_e / (1.0 + jnp.exp(-gate_e))) * up_e).astype(bf16)
    up_d = mm(normed, wdu[...])
    hidden_d = (dense * (gate_d / (1.0 + jnp.exp(-gate_d))) * up_d).astype(bf16)
    copies[0].wait()
    copies[1].wait()
    for z in range(chips):
        at = slice(z * lanes, (z + 1) * lanes)
        block = mm(hidden_e, wed[:, at]) + mm(hidden_d, wdd[:, at])
        above, below = block[:rows], block[rows:]
        zero = jnp.where(low, above, pltpu.roll(below, lanes // 2, 1))
        one = jnp.where(low, pltpu.roll(above, lanes // 2, 1), below)
        keep[z] = jnp.where(core == 0, zero, one)
        send[z] = jnp.where(core == 0, one, zero).astype(bf16)
    own = xbuf[:, pl.ds(pl.multiple_of(chip * lanes, lanes), lanes)].astype(f32)
    above, below = own[:rows], own[rows:]
    zero = jnp.where(low, above, pltpu.roll(below, lanes // 2, 1))
    one = jnp.where(low, pltpu.roll(above, lanes // 2, 1), below)
    rest[...] = residual_scale * jnp.where(core == 0, zero, one)


def pair_sum(keep, got, out):
    out[...] = (keep[...] + got[...].astype(f32)).astype(bf16)


def gather_sums(got, rest, final, stats):
    chips, rows, lanes = got.shape
    total = rest[...]
    for z in range(chips):
        total = total + got[z].astype(f32)
    final[...] = total
    low = iota((rows, lanes), 1) < lanes // 2
    lane = iota((rows, lanes), 1)
    sub = iota((rows, lanes), 0)
    square = total * total
    line = jnp.zeros((1, lanes), f32)
    for k, v in enumerate(
        (
            jnp.where(low, total, 0.0),
            jnp.where(low, 0.0, total),
            jnp.where(low, square, 0.0),
            jnp.where(low, 0.0, square),
        )
    ):
        column = jnp.sum(v, axis=1, keepdims=True)
        line = line + jnp.sum(jnp.where(lane == sub + k * rows, column, 0.0), axis=0, keepdims=True)
    for d in range(stats.shape[0]):
        stats[d] = line


def finish(final, stats, gain, out):
    rows, lanes = final.shape
    ranks = stats.shape[0]
    line = stats[0]
    for d in range(1, ranks):
        line = line + stats[d]
    lane = iota((rows, lanes), 1)
    sub = iota((rows, lanes), 0)
    low = lane < lanes // 2
    width = ranks * (lanes // 2)
    columns = [
        jnp.sum(jnp.where(lane == sub + k * rows, line, 0.0), axis=1, keepdims=True) / width
        for k in range(4)
    ]
    center = jnp.where(low, columns[0], columns[1])
    second = jnp.where(low, columns[2], columns[3])
    unit = (final[...] - center) * lax.rsqrt(second - center * center + norm_eps)
    stacked = jnp.concatenate([unit[:, : lanes // 2], unit[:, lanes // 2 :]], axis=0)
    stacked = (stacked * gain[...].reshape(1, lanes // 2).astype(f32)).astype(bf16)
    seqs = stacked.shape[0]
    here = seqs // ranks
    s = iota((seqs, seqs), 0)
    inside = lax.rem(s, CORES * here)
    source = (inside // here) * rows + (s // (CORES * here)) * here + lax.rem(inside, here)
    place = (iota((seqs, seqs), 1) == source).astype(f32).astype(bf16)
    out[...] = mm(place, stacked).astype(bf16)


def shards(
    tokens,
    w_query,
    w_key,
    w_value,
    w_forget,
    forget_bias,
    cache_keys,
    cache_values,
    cache_gates,
    lengths,
    w_out,
    norm_gain,
    w_router,
    routes,
    dense_gate,
    dense_w_gate,
    dense_w_up,
    dense_w_down,
    expert_w_gate,
    expert_w_up,
    expert_w_down,
    final_gain,
):
    ranks = lax.axis_size("ep")
    chips = ranks // CORES
    seqs, feats = tokens.shape
    here = seqs // ranks
    rows = seqs // CORES
    width = w_query.shape[1]
    heads = w_forget.shape[1]
    places = cache_keys.shape[1]
    model = w_out.shape[1]
    planes = [[CORES * z + c for z in range(chips)] for c in range(CORES)]
    pairs = [(i, i ^ 1) for i in range(ranks)]
    sds = jax.ShapeDtypeStruct

    def far(arrays):
        return tuple(pltpu.with_memory_space_constraint(a, HBM) for a in arrays)

    def swap(a):
        return lax.ppermute(a, "ep", pairs)

    def exchange(a):
        return lax.all_to_all(
            a, "ep", split_axis=0, concat_axis=0, tiled=True, axis_index_groups=planes
        )

    dma = pltpu.SemaphoreType.DMA
    wf = jnp.transpose(w_forget)
    sent = (tokens, w_query, w_key, w_value, wf)
    arrived = tuple(swap(a) for a in sent)
    partial, own, w_pairs = call(
        project_own,
        (
            sds((rows, 3 * width + LANES), f32),
            sds((rows, feats), bf16),
            sds((w_out.shape[0] // here, here, model), bf16),
        ),
        [whole(HBM)] * 6,
        [VM(a.shape, bf16) for a in (*sent, w_out)] + [dma((6,))],
        limit=6 << 20,
    )(*far((*sent, w_out)))
    terms, tok = call(
        project_pair,
        (
            sds((chips, here, 3 * width + LANES + w_out.shape[0] // here * LANES), bf16),
            sds((rows, LANES), f32),
        ),
        [whole()] * 8,
        limit=6 << 20,
    )(partial, own, w_pairs, *arrived)
    sums = exchange(terms)
    wown = call(
        unpack_columns,
        sds((chips, w_out.shape[0], LANES), bf16),
        [whole()],
        limit=4 << 20,
    )(sums)
    attn = call(
        attention,
        sds((chips, here, width), bf16),
        [whole()] * 2 + [whole(HBM)] * 4,
        [
            pltpu.SMEM((here,), jnp.int32),
            VM((here, heads, places), f32),
            VM((here, places, width), bf16),
            VM((here, places, width), bf16),
            dma((3, 2)),
        ],
        limit=14 << 20,
    )(
        sums,
        forget_bias[None],
        *far((lengths, jnp.transpose(cache_gates, (0, 2, 1)), cache_keys, cache_values)),
    )
    attn_all = exchange(attn)
    wpar = swap(wown)
    mixed = call(
        out_project,
        sds((chips, rows, LANES), bf16),
        [whole()] * 4,
        [VM((width, LANES), bf16)],
        limit=4 << 20,
    )(attn_all, wown, wpar, tok)
    xown = exchange(mixed)
    xpar = swap(xown)
    weights = far(
        (expert_w_gate, dense_w_gate, expert_w_up, dense_w_up, expert_w_down, dense_w_down)
    )
    first = call(
        load_all,
        tuple(VM(w.shape, bf16) for w in weights[:2]),
        [whole(HBM)] * 2,
        [dma((2,))],
        limit=4 << 20,
    )(*weights[:2])
    ups = call(
        load_all,
        tuple(VM(w.shape, bf16) for w in weights[2:4]),
        [whole(HBM)] * 2,
        [dma((2,))],
        limit=4 << 20,
    )(*weights[2:4])
    keep, send, rest = call(
        feed_forward,
        (
            sds((chips, rows, LANES), f32),
            sds((chips, rows, LANES), bf16),
            sds((rows, LANES), f32),
        ),
        [whole()] * 10 + [whole(HBM)] * 2,
        [VM((seqs, model), bf16)] + [VM(w.shape, bf16) for w in weights[4:]] + [dma((2,))],
        limit=18 << 20,
    )(
        xown,
        xpar,
        norm_gain.reshape(chips, LANES),
        dense_gate.reshape(chips, LANES),
        jnp.transpose(w_router),
        jnp.transpose(routes),
        *first,
        *ups,
        *weights[4:],
    )
    part = call(pair_sum, sds((chips, rows, LANES), bf16), [whole()] * 2, limit=4 << 20)(
        keep, swap(send)
    )
    final, stats = call(
        gather_sums,
        (sds((rows, LANES), f32), sds((ranks, 1, LANES), f32)),
        [whole()] * 2,
        limit=4 << 20,
    )(exchange(part), rest)
    stats = lax.all_to_all(stats, "ep", split_axis=0, concat_axis=0, tiled=True)
    return call(finish, sds((seqs, feats), bf16), [whole()] * 3, limit=4 << 20)(
        final, stats, final_gain
    )


def solution(mesh):
    placed = (
        P("grp", "ep"),
        P("ep", None),
        P("ep", None),
        P("ep", None),
        P("ep", None),
        P(),
        P(("grp", "ep"), None, None),
        P(("grp", "ep"), None, None),
        P(("grp", "ep"), None, None),
        P(("grp", "ep")),
        P("ep", None),
        P(),
        P(),
        P("grp", None),
        P(),
        P(None, "ep"),
        P(None, "ep"),
        P("ep", None),
        P(None, "ep"),
        P(None, "ep"),
        P("ep", None),
        P("ep"),
    )

    return jax.shard_map(
        shards, mesh=mesh, in_specs=placed, out_specs=P("grp", "ep"), check_vma=False
    )
```

```python
import jax
import jax.numpy as jnp
from jax import lax
from jax.experimental import pallas as pl
from jax.experimental.pallas import tpu as pltpu
from jax.sharding import PartitionSpec as P


norm_eps = 1e-05
residual_scale = 8.0**0.25
CORES = 2
LANES = 128
bf16 = jnp.bfloat16
f32 = jnp.float32
VM = pltpu.VMEM
HBM = pltpu.HBM


def whole(space=VM):
    return pl.BlockSpec(memory_space=space)


def call(kernel, outs, ins, scratch=(), limit=None):
    return pl.pallas_call(
        kernel,
        out_shape=outs,
        in_specs=ins,
        out_specs=jax.tree.map(lambda _: whole(), outs),
        scratch_shapes=list(scratch),
        compiler_params=pltpu.CompilerParams(vmem_limit_bytes=limit),
    )


def iota(shape, dim):
    return lax.broadcasted_iota(jnp.int32, shape, dim)


def nt(a, b):
    return lax.dot_general(a, b, (((1,), (1,)), ((), ())), preferred_element_type=f32)


def mm(a, b):
    return jnp.dot(a, b, preferred_element_type=f32)


def my_half():
    return lax.rem(lax.axis_index("grp"), 2)


def plane_rows(rows, seqs, here):
    core = lax.rem(lax.axis_index("ep"), CORES)
    r = iota((rows, seqs), 0)
    source = (r // here) * (CORES * here) + core * here + lax.rem(r, here)
    return (iota((rows, seqs), 1) == source).astype(f32).astype(bf16)


def project_own(
    tok_hbm, wq_hbm, wk_hbm, wv_hbm, wf_hbm, wout_hbm,
    partial, own_out, pairs, tok, wq, wk, wv, wf, wout, sems,
):
    share = wout.shape[0]
    copies = [
        pltpu.make_async_copy(src, dst, sems.at[k])
        for k, (src, dst) in enumerate(
            (
                (tok_hbm, tok),
                (wq_hbm, wq),
                (wk_hbm, wk),
                (wv_hbm, wv),
                (wf_hbm, wf),
                (wout_hbm.at[pl.ds(pl.multiple_of(my_half() * share, share), share)], wout),
            )
        )
    ]
    for c in copies:
        c.start()
    rows = own_out.shape[0]
    pick = plane_rows(rows, tok.shape[0], pairs.shape[1])
    for c in copies:
        c.wait()
    own = mm(pick, tok[...]).astype(bf16)
    own_out[...] = own
    width = wq.shape[1]
    for k, w in enumerate((wq, wk, wv)):
        partial[:, k * width : (k + 1) * width] = mm(own, w[...])
    forget = nt(own, wf[...])
    heads = wf.shape[0]
    pad = jnp.zeros((rows, LANES - 2 * heads), f32)
    partial[:, 3 * width :] = jnp.concatenate([forget, forget, pad], axis=1)
    pairs[...] = wout[...].reshape(pairs.shape)


def project_pair(partial, own, pairs, tokp, pq, pk, pv, pf, out, tok_out):
    core = lax.rem(lax.axis_index("ep"), CORES)
    dest, here, _ = out.shape
    rows = own.shape[0]
    other = mm(plane_rows(rows, tokp.shape[0], here), tokp[...]).astype(bf16)
    width = pq.shape[1]
    for k, p in enumerate((pq, pk, pv)):
        at = slice(k * width, (k + 1) * width)
        term = partial[:, at] + mm(other, p[...])
        out[:, :, at] = term.reshape(dest, here, width).astype(bf16)
    heads = pf.shape[0]
    forget = nt(other, pf[...])
    pad = jnp.zeros((rows, LANES - 2 * heads), f32)
    both = partial[:, 3 * width :] + jnp.concatenate([forget, forget, pad], axis=1)
    high = both.astype(bf16).astype(f32)
    both = jnp.where(iota(both.shape, 1) < heads, high, both - high)
    out[:, :, 3 * width : 3 * width + LANES] = both.reshape(dest, here, LANES).astype(bf16)
    mine = own[...].astype(f32)
    other = other.astype(f32)
    first = jnp.where(core == 0, mine, other)
    second = jnp.where(core == 0, other, mine)
    tok_out[...] = jnp.concatenate([first, second], axis=1)
    base = 3 * width + LANES
    for z in range(dest):
        for t in range(pairs.shape[0]):
            out[z, :, base + t * LANES : base + (t + 1) * LANES] = pairs[
                t, :, z * LANES : (z + 1) * LANES
            ]


def unpack_columns(got, out):
    dest, here, _ = got.shape
    steps = out.shape[1] // here
    base = got.shape[2] - steps * LANES
    for z in range(dest):
        out[z] = jnp.concatenate(
            [
                got[z, :, base + t * LANES : base + (t + 1) * LANES].astype(f32)
                for t in range(steps)
            ],
            axis=0,
        ).astype(bf16)


def load_all(*refs):
    count = len(refs) // 2
    sems = refs[-1]
    copies = [
        pltpu.make_async_copy(refs[k], refs[count + k], sems.at[k]) for k in range(count)
    ]
    for c in copies:
        c.start()
    for c in copies:
        c.wait()


def attention(
    got, forget_hbm, lengths_hbm, gates_hbm, keys_hbm, values_hbm, out,
    forget_bias, lengths, gates, keys, values, sems,
):
    dest, here, _ = got.shape
    heads, places = gates.shape[1:]
    width = keys.shape[2]
    small = [
        pltpu.make_async_copy(lengths_hbm, lengths, sems.at[2, 0]),
        pltpu.make_async_copy(gates_hbm, gates, sems.at[2, 1]),
        pltpu.make_async_copy(forget_hbm, forget_bias, sems.at[3, 0]),
    ]
    kcopy = [pltpu.make_async_copy(keys_hbm.at[j], keys.at[j], sems.at[0, j]) for j in range(here)]
    vcopy = [
        pltpu.make_async_copy(values_hbm.at[j], values.at[j], sems.at[1, j]) for j in range(here)
    ]
    for c in small + kcopy + vcopy:
        c.start()
    size = width // heads
    used = 3 * width + LANES
    total = got[0, :, :used].astype(f32)
    for z in range(1, dest):
        total = total + got[z, :, :used].astype(f32)
    mine = iota((heads, width), 1) // size == iota((heads, width), 0)
    lane = iota((heads, LANES), 1)
    sub = iota((heads, LANES), 0)
    scale = size**-0.5
    position = iota((heads, places), 1)
    for c in small:
        c.wait()
    added = jnp.zeros((heads, 1), f32)
    for h in range(heads):
        added = jnp.where(iota((heads, 1), 0) == h, forget_bias[h], added)
    soft = []
    for j in range(here):
        row = total[j : j + 1]
        query = jnp.where(mine, row[:, :width].astype(bf16).astype(f32), 0.0)
        new_key = row[:, width : 2 * width].astype(bf16).astype(f32)
        tail = row[:, 3 * width : 3 * width + LANES]
        forget = jnp.sum(
            jnp.where((lane == sub) | (lane == sub + heads), tail, 0.0), axis=1, keepdims=True
        )
        x = forget + added
        log_gate = -(jnp.maximum(-x, 0.0) + jnp.log1p(jnp.exp(-jnp.abs(x))))
        own = jnp.sum(query * new_key, axis=1, keepdims=True) * scale
        gate = gates[j]
        length = lengths[j]
        last = jnp.sum(jnp.where(position == length - 1, gate, 0.0), axis=1, keepdims=True)
        bias = jnp.where(position < length, (last + log_gate) - gate, -jnp.inf)
        kcopy[j].wait()
        scores = nt(query.astype(bf16), keys[j]) * scale + bias
        top = jnp.maximum(jnp.max(scores, axis=1, keepdims=True), own)
        weights = jnp.exp(scores - top)
        weight_own = jnp.exp(own - top)
        sums = jnp.sum(weights, axis=1, keepdims=True) + weight_own
        soft.append(((weights / sums).astype(bf16), (weight_own / sums).astype(bf16).astype(f32)))
    rows = []
    for j in range(here):
        probs, prob_own = soft[j]
        vcopy[j].wait()
        new_value = total[j : j + 1, 2 * width : 3 * width].astype(bf16).astype(f32)
        mixed = mm(probs, values[j]) + prob_own * new_value
        rows.append(jnp.sum(jnp.where(mine, mixed, 0.0), axis=0, keepdims=True))
    attn = jnp.concatenate(rows, axis=0).astype(bf16)
    for z in range(dest):
        out[z] = attn


def out_project(got, own, other, own_par, other_par, tok, out, wbuf):
    core = lax.rem(lax.axis_index("ep"), CORES)
    half = my_half()
    dest, here, width = got.shape
    part = own.shape[1]
    for z in range(dest):
        for side, near, across in ((core, own, other), (1 - core, own_par, other_par)):
            base = (z * CORES + side) * 2 * part
            wbuf[pl.ds(pl.multiple_of(base + half * part, part), part), :] = near[z]
            wbuf[pl.ds(pl.multiple_of(base + (1 - half) * part, part), part), :] = across[z]
    attn = got[...].astype(f32).reshape(dest * here, width).astype(bf16)
    mixed = (mm(attn, wbuf[...]) + residual_scale * tok[...]).astype(bf16)
    for z in range(dest):
        out[z] = mixed


def feed_forward(
    xown, xpar, gain, shutter, router, routes, weg, wdg, weu, wdu,
    wed_hbm, wdd_hbm,
    keep, send, rest,
    xbuf, wed, wdd, sems,
):
    rank = lax.axis_index("ep")
    ranks = lax.axis_size("ep")
    core = lax.rem(rank, CORES)
    copies = [
        pltpu.make_async_copy(src, dst, sems.at[k])
        for k, (src, dst) in enumerate(
            ((wed_hbm, wed), (wdd_hbm, wdd))
        )
    ]
    for c in copies:
        c.start()
    chips, rows, lanes = xown.shape
    width = chips * lanes
    seqs = CORES * rows
    here = seqs // ranks
    experts = router.shape[0]
    low = iota((rows, lanes), 1) < lanes // 2
    chip = rank // CORES
    for half, ref in ((core, xown), (1 - core, xpar)):
        x = ref[...].astype(f32)
        ones = jnp.sum(x, axis=0)
        squares = jnp.sum(x * x, axis=0)
        center = jnp.sum(ones, axis=1, keepdims=True) / width
        second = jnp.sum(squares, axis=1, keepdims=True) / width
        factor = lax.rsqrt(second - center * center + norm_eps)
        for z in range(chips):
            block = (x[z] - center) * factor * gain[z : z + 1, :].astype(f32)
            xbuf[pl.ds(pl.multiple_of(half * rows, rows), rows), z * lanes : (z + 1) * lanes] = (
                block.astype(bf16)
            )
    normed = xbuf[...]
    logits = nt(normed, router[...])
    slot = iota(logits.shape, 1)
    r = iota((seqs, seqs), 0)
    inside = lax.rem(r, rows)
    source = (inside // here) * (CORES * here) + (r // rows) * here + lax.rem(inside, here)
    same = iota((seqs, seqs), 1) == source
    route0 = jnp.sum(jnp.where(same, routes[0:1, :], 0), axis=1, keepdims=True)
    route1 = jnp.sum(jnp.where(same, routes[1:2, :], 0), axis=1, keepdims=True)
    logit0 = jnp.sum(jnp.where(slot == route0, logits, 0.0), axis=1, keepdims=True)
    logit1 = jnp.sum(jnp.where(slot == route1, logits, 0.0), axis=1, keepdims=True)
    peak = jnp.maximum(logit0, logit1)
    e0, e1 = jnp.exp(logit0 - peak), jnp.exp(logit1 - peak)
    expert = rank // (ranks // experts)
    weight = (jnp.where(route0 == expert, e0, 0.0) + jnp.where(route1 == expert, e1, 0.0)) / (e0 + e1)
    shut = jnp.zeros((seqs, lanes), f32)
    for z in range(chips):
        block = xbuf[:, z * lanes : (z + 1) * lanes].astype(f32)
        shut = shut + block * shutter[z : z + 1, :].astype(f32)
    shut = jnp.sum(shut, axis=1, keepdims=True)
    dense = 1.0 / (1.0 + jnp.exp(-shut))
    gate_e = mm(normed, weg[...])
    gate_d = mm(normed, wdg[...])
    up_e = mm(normed, weu[...])
    hidden_e = (weight * (gate_e / (1.0 + jnp.exp(-gate_e))) * up_e).astype(bf16)
    up_d = mm(normed, wdu[...])
    hidden_d = (dense * (gate_d / (1.0 + jnp.exp(-gate_d))) * up_d).astype(bf16)
    copies[0].wait()
    copies[1].wait()
    for z in range(chips):
        at = slice(z * lanes, (z + 1) * lanes)
        block = mm(hidden_e, wed[:, at]) + mm(hidden_d, wdd[:, at])
        above, below = block[:rows], block[rows:]
        zero = jnp.where(low, above, pltpu.roll(below, lanes // 2, 1))
        one = jnp.where(low, pltpu.roll(above, lanes // 2, 1), below)
        keep[z] = jnp.where(core == 0, zero, one)
        send[z] = jnp.where(core == 0, one, zero).astype(bf16)
    own = xbuf[:, pl.ds(pl.multiple_of(chip * lanes, lanes), lanes)].astype(f32)
    above, below = own[:rows], own[rows:]
    zero = jnp.where(low, above, pltpu.roll(below, lanes // 2, 1))
    one = jnp.where(low, pltpu.roll(above, lanes // 2, 1), below)
    rest[...] = residual_scale * jnp.where(core == 0, zero, one)


def pair_sum(keep, got, out):
    out[...] = (keep[...] + got[...].astype(f32)).astype(bf16)


def gather_sums(got, rest, final, stats):
    chips, rows, lanes = got.shape
    total = rest[...]
    for z in range(chips):
        total = total + got[z].astype(f32)
    final[...] = total
    low = iota((rows, lanes), 1) < lanes // 2
    lane = iota((rows, lanes), 1)
    sub = iota((rows, lanes), 0)
    square = total * total
    line = jnp.zeros((1, lanes), f32)
    for k, v in enumerate(
        (
            jnp.where(low, total, 0.0),
            jnp.where(low, 0.0, total),
            jnp.where(low, square, 0.0),
            jnp.where(low, 0.0, square),
        )
    ):
        column = jnp.sum(v, axis=1, keepdims=True)
        line = line + jnp.sum(jnp.where(lane == sub + k * rows, column, 0.0), axis=0, keepdims=True)
    for d in range(stats.shape[0]):
        stats[d] = line


def finish(final, stats, gain, out):
    rows, lanes = final.shape
    ranks = stats.shape[0]
    line = stats[0]
    for d in range(1, ranks):
        line = line + stats[d]
    lane = iota((rows, lanes), 1)
    sub = iota((rows, lanes), 0)
    low = lane < lanes // 2
    width = ranks * (lanes // 2)
    columns = [
        jnp.sum(jnp.where(lane == sub + k * rows, line, 0.0), axis=1, keepdims=True) / width
        for k in range(4)
    ]
    center = jnp.where(low, columns[0], columns[1])
    second = jnp.where(low, columns[2], columns[3])
    unit = (final[...] - center) * lax.rsqrt(second - center * center + norm_eps)
    stacked = jnp.concatenate([unit[:, : lanes // 2], unit[:, lanes // 2 :]], axis=0)
    stacked = (stacked * gain[...].reshape(1, lanes // 2).astype(f32)).astype(bf16)
    seqs = stacked.shape[0]
    here = seqs // ranks
    s = iota((seqs, seqs), 0)
    inside = lax.rem(s, CORES * here)
    source = (inside // here) * rows + (s // (CORES * here)) * here + lax.rem(inside, here)
    place = (iota((seqs, seqs), 1) == source).astype(f32).astype(bf16)
    out[...] = mm(place, stacked).astype(bf16)


def shards(
    tokens,
    w_query,
    w_key,
    w_value,
    w_forget,
    forget_bias,
    cache_keys,
    cache_values,
    cache_gates,
    lengths,
    w_out,
    norm_gain,
    w_router,
    routes,
    dense_gate,
    dense_w_gate,
    dense_w_up,
    dense_w_down,
    expert_w_gate,
    expert_w_up,
    expert_w_down,
    final_gain,
):
    ranks = lax.axis_size("ep")
    chips = ranks // CORES
    seqs, feats = tokens.shape
    here = seqs // ranks
    rows = seqs // CORES
    width = w_query.shape[1]
    heads = w_forget.shape[1]
    places = cache_keys.shape[1]
    model = w_out.shape[1]
    planes = [[CORES * z + c for z in range(chips)] for c in range(CORES)]
    pairs = [(i, i ^ 1) for i in range(ranks)]
    sds = jax.ShapeDtypeStruct
    half_rows = w_out.shape[0] // 2

    def far(arrays):
        return tuple(pltpu.with_memory_space_constraint(a, HBM) for a in arrays)

    def swap(a):
        return lax.ppermute(a, "ep", pairs)

    def exchange(a):
        return lax.all_to_all(
            a, "ep", split_axis=0, concat_axis=0, tiled=True, axis_index_groups=planes
        )

    dma = pltpu.SemaphoreType.DMA
    wf = jnp.transpose(w_forget)
    sent = (tokens, w_query, w_key, w_value, wf)
    arrived = tuple(swap(a) for a in sent)
    partial, own, w_pairs = call(
        project_own,
        (
            sds((rows, 3 * width + LANES), f32),
            sds((rows, feats), bf16),
            sds((half_rows // here, here, model), bf16),
        ),
        [whole(HBM)] * 6,
        [VM(a.shape, bf16) for a in sent] + [VM((half_rows, model), bf16), dma((6,))],
        limit=6 << 20,
    )(*far((*sent, w_out)))
    terms, tok = call(
        project_pair,
        (
            sds((chips, here, 3 * width + LANES + half_rows // here * LANES), bf16),
            sds((rows, LANES), f32),
        ),
        [whole()] * 8,
        limit=6 << 20,
    )(partial, own, w_pairs, *arrived)
    sums = exchange(terms)
    wown = call(
        unpack_columns,
        sds((chips, half_rows, LANES), bf16),
        [whole()],
        limit=4 << 20,
    )(sums)
    attn = call(
        attention,
        sds((chips, here, width), bf16),
        [whole()] + [whole(HBM)] * 5,
        [
            pltpu.SMEM((heads,), f32),
            pltpu.SMEM((here,), jnp.int32),
            VM((here, heads, places), f32),
            VM((here, places, width), bf16),
            VM((here, places, width), bf16),
            dma((4, here)),
        ],
        limit=14 << 20,
    )(
        sums,
        *far((forget_bias, lengths, jnp.transpose(cache_gates, (0, 2, 1)), cache_keys, cache_values)),
    )
    attn_all = exchange(attn)
    groups = lax.axis_size("grp")
    wother = lax.ppermute(wown, "grp", [(g, g ^ 1) for g in range(groups)])
    wother_par = lax.ppermute(
        wown,
        ("grp", "ep"),
        [(g * ranks + i, (g ^ 1) * ranks + (i ^ 1)) for g in range(groups) for i in range(ranks)],
    )
    wpar = swap(wown)
    mixed = call(
        out_project,
        sds((chips, rows, LANES), bf16),
        [whole()] * 6,
        [VM((width, LANES), bf16)],
        limit=4 << 20,
    )(attn_all, wown, wother, wpar, wother_par, tok)
    xown = exchange(mixed)
    xpar = swap(xown)
    weights = far(
        (expert_w_gate, dense_w_gate, expert_w_up, dense_w_up, expert_w_down, dense_w_down)
    )
    first = call(
        load_all,
        tuple(VM(w.shape, bf16) for w in weights[:2]),
        [whole(HBM)] * 2,
        [dma((2,))],
        limit=4 << 20,
    )(*weights[:2])
    ups = call(
        load_all,
        tuple(VM(w.shape, bf16) for w in weights[2:4]),
        [whole(HBM)] * 2,
        [dma((2,))],
        limit=4 << 20,
    )(*weights[2:4])
    keep, send, rest = call(
        feed_forward,
        (
            sds((chips, rows, LANES), f32),
            sds((chips, rows, LANES), bf16),
            sds((rows, LANES), f32),
        ),
        [whole()] * 10 + [whole(HBM)] * 2,
        [VM((seqs, model), bf16)] + [VM(w.shape, bf16) for w in weights[4:]] + [dma((2,))],
        limit=18 << 20,
    )(
        xown,
        xpar,
        norm_gain.reshape(chips, LANES),
        dense_gate.reshape(chips, LANES),
        jnp.transpose(w_router),
        jnp.transpose(routes),
        *first,
        *ups,
        *weights[4:],
    )
    part = call(pair_sum, sds((chips, rows, LANES), bf16), [whole()] * 2, limit=4 << 20)(
        keep, swap(send)
    )
    final, stats = call(
        gather_sums,
        (sds((rows, LANES), f32), sds((ranks, 1, LANES), f32)),
        [whole()] * 2,
        limit=4 << 20,
    )(exchange(part), rest)
    stats = lax.all_to_all(stats, "ep", split_axis=0, concat_axis=0, tiled=True)
    return call(finish, sds((seqs, feats), bf16), [whole()] * 3, limit=4 << 20)(
        final, stats, final_gain
    )


def solution(mesh):
    placed = (
        P("grp", "ep"),
        P("ep", None),
        P("ep", None),
        P("ep", None),
        P("ep", None),
        P(),
        P(("grp", "ep"), None, None),
        P(("grp", "ep"), None, None),
        P(("grp", "ep"), None, None),
        P(("grp", "ep")),
        P("ep", None),
        P(),
        P(),
        P("grp", None),
        P(),
        P(None, "ep"),
        P(None, "ep"),
        P("ep", None),
        P(None, "ep"),
        P(None, "ep"),
        P("ep", None),
        P("ep"),
    )

    return jax.shard_map(
        shards, mesh=mesh, in_specs=placed, out_specs=P("grp", "ep"), check_vma=False
    )
```

```python
import jax
import jax.numpy as jnp
from jax import lax
from jax.experimental import pallas as pl
from jax.experimental.pallas import tpu as pltpu
from jax.sharding import PartitionSpec as P


norm_eps = 1e-05
residual_scale = 8.0**0.25
CORES = 2
LANES = 128
bf16 = jnp.bfloat16
f32 = jnp.float32
VM = pltpu.VMEM
HBM = pltpu.HBM


def whole(space=VM):
    return pl.BlockSpec(memory_space=space)


def call(kernel, outs, ins, scratch=(), limit=None):
    return pl.pallas_call(
        kernel,
        out_shape=outs,
        in_specs=ins,
        out_specs=jax.tree.map(lambda _: whole(), outs),
        scratch_shapes=list(scratch),
        compiler_params=pltpu.CompilerParams(vmem_limit_bytes=limit),
    )


def iota(shape, dim):
    return lax.broadcasted_iota(jnp.int32, shape, dim)


def nt(a, b):
    return lax.dot_general(a, b, (((1,), (1,)), ((), ())), preferred_element_type=f32)


def mm(a, b):
    return jnp.dot(a, b, preferred_element_type=f32)


def my_half():
    return lax.rem(lax.axis_index("grp"), 2)


def plane_rows(rows, seqs, here):
    core = lax.rem(lax.axis_index("ep"), CORES)
    r = iota((rows, seqs), 0)
    source = (r // here) * (CORES * here) + core * here + lax.rem(r, here)
    return (iota((rows, seqs), 1) == source).astype(f32).astype(bf16)


def project_own(
    tok_hbm, wq_hbm, wk_hbm, wv_hbm, wf_hbm, wout_hbm, keys_hbm,
    partial, own_out, pairs, first, tok, wq, wk, wv, wf, wout, sems,
):
    share = wout.shape[0]
    copies = [
        pltpu.make_async_copy(src, dst, sems.at[k])
        for k, (src, dst) in enumerate(
            (
                (tok_hbm, tok),
                (wq_hbm, wq),
                (wk_hbm, wk),
                (wv_hbm, wv),
                (wf_hbm, wf),
                (wout_hbm.at[pl.ds(pl.multiple_of(my_half() * share, share), share)], wout),
            )
        )
    ]
    for c in copies:
        c.start()
    keys_copy = pltpu.make_async_copy(keys_hbm.at[0], first, sems.at[len(copies)])
    keys_copy.start()
    rows = own_out.shape[0]
    pick = plane_rows(rows, tok.shape[0], pairs.shape[1])
    for c in copies:
        c.wait()
    own = mm(pick, tok[...]).astype(bf16)
    own_out[...] = own
    width = wq.shape[1]
    for k, w in enumerate((wq, wk, wv)):
        partial[:, k * width : (k + 1) * width] = mm(own, w[...])
    forget = nt(own, wf[...])
    heads = wf.shape[0]
    pad = jnp.zeros((rows, LANES - 2 * heads), f32)
    partial[:, 3 * width :] = jnp.concatenate([forget, forget, pad], axis=1)
    pairs[...] = wout[...].reshape(pairs.shape)
    keys_copy.wait()


def project_pair(partial, own, pairs, tokp, pq, pk, pv, pf, out, tok_out):
    core = lax.rem(lax.axis_index("ep"), CORES)
    dest, here, _ = out.shape
    rows = own.shape[0]
    other = mm(plane_rows(rows, tokp.shape[0], here), tokp[...]).astype(bf16)
    width = pq.shape[1]
    for k, p in enumerate((pq, pk, pv)):
        at = slice(k * width, (k + 1) * width)
        term = partial[:, at] + mm(other, p[...])
        out[:, :, at] = term.reshape(dest, here, width).astype(bf16)
    heads = pf.shape[0]
    forget = nt(other, pf[...])
    pad = jnp.zeros((rows, LANES - 2 * heads), f32)
    both = partial[:, 3 * width :] + jnp.concatenate([forget, forget, pad], axis=1)
    high = both.astype(bf16).astype(f32)
    both = jnp.where(iota(both.shape, 1) < heads, high, both - high)
    out[:, :, 3 * width : 3 * width + LANES] = both.reshape(dest, here, LANES).astype(bf16)
    mine = own[...].astype(f32)
    other = other.astype(f32)
    first = jnp.where(core == 0, mine, other)
    second = jnp.where(core == 0, other, mine)
    tok_out[...] = jnp.concatenate([first, second], axis=1)
    base = 3 * width + LANES
    for z in range(dest):
        for t in range(pairs.shape[0]):
            out[z, :, base + t * LANES : base + (t + 1) * LANES] = pairs[
                t, :, z * LANES : (z + 1) * LANES
            ]


def unpack_columns(got, out):
    dest, here, _ = got.shape
    steps = out.shape[1] // here
    base = got.shape[2] - steps * LANES
    for z in range(dest):
        out[z] = jnp.concatenate(
            [
                got[z, :, base + t * LANES : base + (t + 1) * LANES].astype(f32)
                for t in range(steps)
            ],
            axis=0,
        ).astype(bf16)


def load_all(*refs):
    count = len(refs) // 2
    sems = refs[-1]
    copies = [
        pltpu.make_async_copy(refs[k], refs[count + k], sems.at[k]) for k in range(count)
    ]
    for c in copies:
        c.start()
    for c in copies:
        c.wait()


def attention(
    got, first, forget_hbm, lengths_hbm, gates_hbm, keys_hbm, values_hbm, out,
    forget_bias, lengths, gates, keys, values, sems,
):
    dest, here, _ = got.shape
    heads, places = gates.shape[1:]
    width = keys.shape[2]
    small = [
        pltpu.make_async_copy(lengths_hbm, lengths, sems.at[2, 0]),
        pltpu.make_async_copy(gates_hbm, gates, sems.at[2, 1]),
        pltpu.make_async_copy(forget_hbm, forget_bias, sems.at[3, 0]),
    ]
    kcopy = [pltpu.make_async_copy(keys_hbm.at[j], keys.at[j - 1], sems.at[0, j]) for j in range(1, here)]
    vcopy = [
        pltpu.make_async_copy(values_hbm.at[j], values.at[j], sems.at[1, j]) for j in range(here)
    ]
    for c in small + kcopy + vcopy:
        c.start()
    size = width // heads
    used = 3 * width + LANES
    total = got[0, :, :used].astype(f32)
    for z in range(1, dest):
        total = total + got[z, :, :used].astype(f32)
    mine = iota((heads, width), 1) // size == iota((heads, width), 0)
    lane = iota((heads, LANES), 1)
    sub = iota((heads, LANES), 0)
    scale = size**-0.5
    position = iota((heads, places), 1)
    for c in small:
        c.wait()
    added = jnp.zeros((heads, 1), f32)
    for h in range(heads):
        added = jnp.where(iota((heads, 1), 0) == h, forget_bias[h], added)
    soft = []
    for j in range(here):
        row = total[j : j + 1]
        query = jnp.where(mine, row[:, :width].astype(bf16).astype(f32), 0.0)
        new_key = row[:, width : 2 * width].astype(bf16).astype(f32)
        tail = row[:, 3 * width : 3 * width + LANES]
        forget = jnp.sum(
            jnp.where((lane == sub) | (lane == sub + heads), tail, 0.0), axis=1, keepdims=True
        )
        x = forget + added
        log_gate = -(jnp.maximum(-x, 0.0) + jnp.log1p(jnp.exp(-jnp.abs(x))))
        own = jnp.sum(query * new_key, axis=1, keepdims=True) * scale
        gate = gates[j]
        length = lengths[j]
        last = jnp.sum(jnp.where(position == length - 1, gate, 0.0), axis=1, keepdims=True)
        bias = jnp.where(position < length, (last + log_gate) - gate, -jnp.inf)
        if j > 0:
            kcopy[j - 1].wait()
        keys_here = first[...] if j == 0 else keys[j - 1]
        scores = nt(query.astype(bf16), keys_here) * scale + bias
        top = jnp.maximum(jnp.max(scores, axis=1, keepdims=True), own)
        weights = jnp.exp(scores - top)
        weight_own = jnp.exp(own - top)
        sums = jnp.sum(weights, axis=1, keepdims=True) + weight_own
        soft.append(((weights / sums).astype(bf16), (weight_own / sums).astype(bf16).astype(f32)))
    rows = []
    for j in range(here):
        probs, prob_own = soft[j]
        vcopy[j].wait()
        new_value = total[j : j + 1, 2 * width : 3 * width].astype(bf16).astype(f32)
        mixed = mm(probs, values[j]) + prob_own * new_value
        rows.append(jnp.sum(jnp.where(mine, mixed, 0.0), axis=0, keepdims=True))
    attn = jnp.concatenate(rows, axis=0).astype(bf16)
    for z in range(dest):
        out[z] = attn


def out_project(got, own, other, own_par, other_par, tok, out, wbuf):
    core = lax.rem(lax.axis_index("ep"), CORES)
    half = my_half()
    dest, here, width = got.shape
    part = own.shape[1]
    for z in range(dest):
        for side, near, across in ((core, own, other), (1 - core, own_par, other_par)):
            base = (z * CORES + side) * 2 * part
            wbuf[pl.ds(pl.multiple_of(base + half * part, part), part), :] = near[z]
            wbuf[pl.ds(pl.multiple_of(base + (1 - half) * part, part), part), :] = across[z]
    attn = got[...].astype(f32).reshape(dest * here, width).astype(bf16)
    mixed = (mm(attn, wbuf[...]) + residual_scale * tok[...]).astype(bf16)
    for z in range(dest):
        out[z] = mixed


def feed_forward(
    xown, xpar, gain, shutter, router, routes, weg, wdg, weu, wdu,
    wed_hbm, wdd_hbm,
    keep, send, rest,
    xbuf, wed, wdd, sems,
):
    rank = lax.axis_index("ep")
    ranks = lax.axis_size("ep")
    core = lax.rem(rank, CORES)
    copies = [
        pltpu.make_async_copy(src, dst, sems.at[k])
        for k, (src, dst) in enumerate(
            ((wed_hbm, wed), (wdd_hbm, wdd))
        )
    ]
    for c in copies:
        c.start()
    chips, rows, lanes = xown.shape
    width = chips * lanes
    seqs = CORES * rows
    here = seqs // ranks
    experts = router.shape[0]
    low = iota((rows, lanes), 1) < lanes // 2
    chip = rank // CORES
    for half, ref in ((core, xown), (1 - core, xpar)):
        x = ref[...].astype(f32)
        ones = jnp.sum(x, axis=0)
        squares = jnp.sum(x * x, axis=0)
        center = jnp.sum(ones, axis=1, keepdims=True) / width
        second = jnp.sum(squares, axis=1, keepdims=True) / width
        factor = lax.rsqrt(second - center * center + norm_eps)
        for z in range(chips):
            block = (x[z] - center) * factor * gain[z : z + 1, :].astype(f32)
            xbuf[pl.ds(pl.multiple_of(half * rows, rows), rows), z * lanes : (z + 1) * lanes] = (
                block.astype(bf16)
            )
    normed = xbuf[...]
    logits = nt(normed, router[...])
    slot = iota(logits.shape, 1)
    r = iota((seqs, seqs), 0)
    inside = lax.rem(r, rows)
    source = (inside // here) * (CORES * here) + (r // rows) * here + lax.rem(inside, here)
    same = iota((seqs, seqs), 1) == source
    route0 = jnp.sum(jnp.where(same, routes[0:1, :], 0), axis=1, keepdims=True)
    route1 = jnp.sum(jnp.where(same, routes[1:2, :], 0), axis=1, keepdims=True)
    logit0 = jnp.sum(jnp.where(slot == route0, logits, 0.0), axis=1, keepdims=True)
    logit1 = jnp.sum(jnp.where(slot == route1, logits, 0.0), axis=1, keepdims=True)
    peak = jnp.maximum(logit0, logit1)
    e0, e1 = jnp.exp(logit0 - peak), jnp.exp(logit1 - peak)
    expert = rank // (ranks // experts)
    weight = (jnp.where(route0 == expert, e0, 0.0) + jnp.where(route1 == expert, e1, 0.0)) / (e0 + e1)
    shut = jnp.zeros((seqs, lanes), f32)
    for z in range(chips):
        block = xbuf[:, z * lanes : (z + 1) * lanes].astype(f32)
        shut = shut + block * shutter[z : z + 1, :].astype(f32)
    shut = jnp.sum(shut, axis=1, keepdims=True)
    dense = 1.0 / (1.0 + jnp.exp(-shut))
    gate_e = mm(normed, weg[...])
    gate_d = mm(normed, wdg[...])
    up_e = mm(normed, weu[...])
    hidden_e = (weight * (gate_e / (1.0 + jnp.exp(-gate_e))) * up_e).astype(bf16)
    up_d = mm(normed, wdu[...])
    hidden_d = (dense * (gate_d / (1.0 + jnp.exp(-gate_d))) * up_d).astype(bf16)
    copies[0].wait()
    copies[1].wait()
    for z in range(chips):
        at = slice(z * lanes, (z + 1) * lanes)
        block = mm(hidden_e, wed[:, at]) + mm(hidden_d, wdd[:, at])
        above, below = block[:rows], block[rows:]
        zero = jnp.where(low, above, pltpu.roll(below, lanes // 2, 1))
        one = jnp.where(low, pltpu.roll(above, lanes // 2, 1), below)
        keep[z] = jnp.where(core == 0, zero, one)
        send[z] = jnp.where(core == 0, one, zero).astype(bf16)
    own = xbuf[:, pl.ds(pl.multiple_of(chip * lanes, lanes), lanes)].astype(f32)
    above, below = own[:rows], own[rows:]
    zero = jnp.where(low, above, pltpu.roll(below, lanes // 2, 1))
    one = jnp.where(low, pltpu.roll(above, lanes // 2, 1), below)
    rest[...] = residual_scale * jnp.where(core == 0, zero, one)


def pair_sum(keep, got, out):
    out[...] = (keep[...] + got[...].astype(f32)).astype(bf16)


def gather_sums(got, rest, final, stats):
    chips, rows, lanes = got.shape
    total = rest[...]
    for z in range(chips):
        total = total + got[z].astype(f32)
    final[...] = total
    low = iota((rows, lanes), 1) < lanes // 2
    lane = iota((rows, lanes), 1)
    sub = iota((rows, lanes), 0)
    square = total * total
    line = jnp.zeros((1, lanes), f32)
    for k, v in enumerate(
        (
            jnp.where(low, total, 0.0),
            jnp.where(low, 0.0, total),
            jnp.where(low, square, 0.0),
            jnp.where(low, 0.0, square),
        )
    ):
        column = jnp.sum(v, axis=1, keepdims=True)
        line = line + jnp.sum(jnp.where(lane == sub + k * rows, column, 0.0), axis=0, keepdims=True)
    for d in range(stats.shape[0]):
        stats[d] = line


def finish(final, stats, gain, out):
    rows, lanes = final.shape
    ranks = stats.shape[0]
    line = stats[0]
    for d in range(1, ranks):
        line = line + stats[d]
    lane = iota((rows, lanes), 1)
    sub = iota((rows, lanes), 0)
    low = lane < lanes // 2
    width = ranks * (lanes // 2)
    columns = [
        jnp.sum(jnp.where(lane == sub + k * rows, line, 0.0), axis=1, keepdims=True) / width
        for k in range(4)
    ]
    center = jnp.where(low, columns[0], columns[1])
    second = jnp.where(low, columns[2], columns[3])
    unit = (final[...] - center) * lax.rsqrt(second - center * center + norm_eps)
    stacked = jnp.concatenate([unit[:, : lanes // 2], unit[:, lanes // 2 :]], axis=0)
    stacked = (stacked * gain[...].reshape(1, lanes // 2).astype(f32)).astype(bf16)
    seqs = stacked.shape[0]
    here = seqs // ranks
    s = iota((seqs, seqs), 0)
    inside = lax.rem(s, CORES * here)
    source = (inside // here) * rows + (s // (CORES * here)) * here + lax.rem(inside, here)
    place = (iota((seqs, seqs), 1) == source).astype(f32).astype(bf16)
    out[...] = mm(place, stacked).astype(bf16)


def shards(
    tokens,
    w_query,
    w_key,
    w_value,
    w_forget,
    forget_bias,
    cache_keys,
    cache_values,
    cache_gates,
    lengths,
    w_out,
    norm_gain,
    w_router,
    routes,
    dense_gate,
    dense_w_gate,
    dense_w_up,
    dense_w_down,
    expert_w_gate,
    expert_w_up,
    expert_w_down,
    final_gain,
):
    ranks = lax.axis_size("ep")
    chips = ranks // CORES
    seqs, feats = tokens.shape
    here = seqs // ranks
    rows = seqs // CORES
    width = w_query.shape[1]
    heads = w_forget.shape[1]
    places = cache_keys.shape[1]
    model = w_out.shape[1]
    planes = [[CORES * z + c for z in range(chips)] for c in range(CORES)]
    pairs = [(i, i ^ 1) for i in range(ranks)]
    sds = jax.ShapeDtypeStruct
    half_rows = w_out.shape[0] // 2

    def far(arrays):
        return tuple(pltpu.with_memory_space_constraint(a, HBM) for a in arrays)

    def swap(a):
        return lax.ppermute(a, "ep", pairs)

    def exchange(a):
        return lax.all_to_all(
            a, "ep", split_axis=0, concat_axis=0, tiled=True, axis_index_groups=planes
        )

    dma = pltpu.SemaphoreType.DMA
    wf = jnp.transpose(w_forget)
    sent = (tokens, w_query, w_key, w_value, wf)
    arrived = tuple(swap(a) for a in sent)
    partial, own, w_pairs, first_keys = call(
        project_own,
        (
            sds((rows, 3 * width + LANES), f32),
            sds((rows, feats), bf16),
            sds((half_rows // here, here, model), bf16),
            VM(cache_keys.shape[1:], bf16),
        ),
        [whole(HBM)] * 7,
        [VM(a.shape, bf16) for a in sent] + [VM((half_rows, model), bf16), dma((7,))],
        limit=6 << 20,
    )(*far((*sent, w_out, cache_keys)))
    terms, tok = call(
        project_pair,
        (
            sds((chips, here, 3 * width + LANES + half_rows // here * LANES), bf16),
            sds((rows, LANES), f32),
        ),
        [whole()] * 8,
        limit=6 << 20,
    )(partial, own, w_pairs, *arrived)
    sums = exchange(terms)
    wown = call(
        unpack_columns,
        sds((chips, half_rows, LANES), bf16),
        [whole()],
        limit=4 << 20,
    )(sums)
    attn = call(
        attention,
        sds((chips, here, width), bf16),
        [whole()] * 2 + [whole(HBM)] * 5,
        [
            pltpu.SMEM((heads,), f32),
            pltpu.SMEM((here,), jnp.int32),
            VM((here, heads, places), f32),
            VM((here - 1, places, width), bf16),
            VM((here, places, width), bf16),
            dma((4, here)),
        ],
        limit=14 << 20,
    )(
        sums,
        first_keys,
        *far((forget_bias, lengths, jnp.transpose(cache_gates, (0, 2, 1)), cache_keys, cache_values)),
    )
    attn_all = exchange(attn)
    groups = lax.axis_size("grp")
    wother = lax.ppermute(wown, "grp", [(g, g ^ 1) for g in range(groups)])
    wother_par = lax.ppermute(
        wown,
        ("grp", "ep"),
        [(g * ranks + i, (g ^ 1) * ranks + (i ^ 1)) for g in range(groups) for i in range(ranks)],
    )
    wpar = swap(wown)
    mixed = call(
        out_project,
        sds((chips, rows, LANES), bf16),
        [whole()] * 6,
        [VM((width, LANES), bf16)],
        limit=4 << 20,
    )(attn_all, wown, wother, wpar, wother_par, tok)
    xown = exchange(mixed)
    xpar = swap(xown)
    weights = far(
        (expert_w_gate, dense_w_gate, expert_w_up, dense_w_up, expert_w_down, dense_w_down)
    )
    first = call(
        load_all,
        tuple(VM(w.shape, bf16) for w in weights[:2]),
        [whole(HBM)] * 2,
        [dma((2,))],
        limit=4 << 20,
    )(*weights[:2])
    ups = call(
        load_all,
        tuple(VM(w.shape, bf16) for w in weights[2:4]),
        [whole(HBM)] * 2,
        [dma((2,))],
        limit=4 << 20,
    )(*weights[2:4])
    keep, send, rest = call(
        feed_forward,
        (
            sds((chips, rows, LANES), f32),
            sds((chips, rows, LANES), bf16),
            sds((rows, LANES), f32),
        ),
        [whole()] * 10 + [whole(HBM)] * 2,
        [VM((seqs, model), bf16)] + [VM(w.shape, bf16) for w in weights[4:]] + [dma((2,))],
        limit=18 << 20,
    )(
        xown,
        xpar,
        norm_gain.reshape(chips, LANES),
        dense_gate.reshape(chips, LANES),
        jnp.transpose(w_router),
        jnp.transpose(routes),
        *first,
        *ups,
        *weights[4:],
    )
    part = call(pair_sum, sds((chips, rows, LANES), bf16), [whole()] * 2, limit=4 << 20)(
        keep, swap(send)
    )
    final, stats = call(
        gather_sums,
        (sds((rows, LANES), f32), sds((ranks, 1, LANES), f32)),
        [whole()] * 2,
        limit=4 << 20,
    )(exchange(part), rest)
    stats = lax.all_to_all(stats, "ep", split_axis=0, concat_axis=0, tiled=True)
    return call(finish, sds((seqs, feats), bf16), [whole()] * 3, limit=4 << 20)(
        final, stats, final_gain
    )


def solution(mesh):
    placed = (
        P("grp", "ep"),
        P("ep", None),
        P("ep", None),
        P("ep", None),
        P("ep", None),
        P(),
        P(("grp", "ep"), None, None),
        P(("grp", "ep"), None, None),
        P(("grp", "ep"), None, None),
        P(("grp", "ep")),
        P("ep", None),
        P(),
        P(),
        P("grp", None),
        P(),
        P(None, "ep"),
        P(None, "ep"),
        P("ep", None),
        P(None, "ep"),
        P(None, "ep"),
        P("ep", None),
        P("ep"),
    )

    return jax.shard_map(
        shards, mesh=mesh, in_specs=placed, out_specs=P("grp", "ep"), check_vma=False
    )
```
